32 devices in a mesh: sp: 8 (over z, y), tp: 4 (over x, core).
Axes of the slice: x: 2, y: 2, z: 4, core: 2. Of those that a mesh axis runs over, the one named last changes fastest.
Arguments:
- stream: bfloat16 [1024, 2048], P('sp'), may hold values from -12 to 12
- out_grad: bfloat16 [1024, 2048], P('sp'), may hold values from -6 to 6
- routes: int32 [1024, 2], P('sp'), may hold values from 0 to 7, all different within a row; in each aligned block of 128 rows (0 to 127, 128 to 255, ...) at most 64 rows name the same one
- route_weight: float32 [1024, 2], P('sp'), may hold values from 0.2 to 1
- queries: bfloat16 [1024, 8, 128], P('sp', 'tp'), may hold values from -6 to 6
- key_vectors: bfloat16 [1024, 8, 128], P('sp', 'tp'), may hold values from -6 to 6
- value_vectors: bfloat16 [1024, 8, 256], P('sp', 'tp'), may hold values from -6 to 6
- log_decay: float32 [1024, 8], P('sp', 'tp'), may hold values from -1 to 0
- out_proj: bfloat16 [2048, 2048], P(None, 'tp'), may hold values from -0.125 to 0.125
- gate_weight: bfloat16 [8, 2048, 1024], P('sp', None, 'tp'), may hold values from -0.125 to 0.125
- up_weight: bfloat16 [8, 2048, 1024], P('sp', None, 'tp'), may hold values from -0.125 to 0.125
- down_weight: bfloat16 [8, 1024, 2048], P('sp', 'tp'), may hold values from -0.1875 to 0.1875
Outputs:
- gate_grad: bfloat16 [8, 2048, 1024], P('sp', None, 'tp')
- up_grad: bfloat16 [8, 2048, 1024], P('sp', None, 'tp')
- down_grad: bfloat16 [8, 1024, 2048], P('sp', 'tp')
- proj_grad: float32 [2048, 2048], P('sp', 'tp')
- query_grad: bfloat16 [1024, 8, 128], P('sp', 'tp')
- key_grad: bfloat16 [1024, 8, 128], P('sp', 'tp')
- value_grad: bfloat16 [1024, 8, 256], P('sp', 'tp')
The draws below stay inside these ranges and needn't reach their ends.
Inputs may be any that keep to these rules, and one draw needn't show every extreme that they name: `routes`: each row names two different experts. In each aligned block of 128 rows no expert is named by more than 64 rows, and in some block an expert is named by exactly 64.
All inputs are finite; a program needn't handle non-finite values.
Results may differ from the reference program's by a relative error of at most 0.025.
Values may be sent and summed in bfloat16 or wider, within the bound.
A program may use at most 128 MiB of HBM per device.

```python
import math
import jax
import jax.numpy as jnp
import numpy as np
from jax import lax

D = 2048
RETENTION_HEADS = 8
KD = 128
VD = 256
FF = 1024
TOK_DEV = 128
SEQUENCE_TOKENS = 1024
EXPERTS = 8
CAP = 64
HV = 2048
N_SP = 8
N_TP = 4


def draw_log_decay(key, part):
    random_subkeys = jax.random.split(jax.random.fold_in(key, 7), 7)
    ranking = jax.random.permutation(random_subkeys[0], RETENTION_HEADS)
    slow_rate = jax.random.uniform(random_subkeys[1], (RETENTION_HEADS,), jnp.float32, 0.05, 0.2) / SEQUENCE_TOKENS
    fast_rate = jnp.exp(jax.random.uniform(random_subkeys[2], (RETENTION_HEADS,), jnp.float32, math.log(0.012), math.log(0.025)))
    baseline_decay_rate = jnp.where(ranking < RETENTION_HEADS // 2, fast_rate, slow_rate)
    decay_factor = jnp.exp(jax.random.uniform(random_subkeys[3], (SEQUENCE_TOKENS // TOK_DEV, RETENTION_HEADS), jnp.float32, 0.0, math.log(3.0)))
    decay_factor = jnp.repeat(decay_factor, TOK_DEV, axis=0)
    jitter_amount = jax.random.uniform(random_subkeys[4], (SEQUENCE_TOKENS, RETENTION_HEADS), jnp.float32, 0.6, 1.4)
    spike_location = jax.random.randint(random_subkeys[5], (2, RETENTION_HEADS), 0, SEQUENCE_TOKENS)
    spike_depth = jax.random.uniform(random_subkeys[6], (2, RETENTION_HEADS), jnp.float32, math.log(0.5), math.log(0.8))
    token_position = jnp.arange(SEQUENCE_TOKENS, dtype=jnp.int32)[:, None]
    spike_events = jnp.where(token_position == spike_location[0][None, :], spike_depth[0][None, :], 0.0)
    spike_events = spike_events + jnp.where(token_position == spike_location[1][None, :], spike_depth[1][None, :], 0.0)
    return -(baseline_decay_rate[None, :] * decay_factor * jitter_amount) + spike_events


def strengthened(drawn, own_key, source, target, shards_of, factor):
    def block_of(position):
        return (jnp.arange(drawn.shape[position]) // (drawn.shape[position] // shards_of)).reshape((-1,) + (1,) * (drawn.ndim - 1 - position))

    first = jax.random.permutation(own_key, shards_of)[block_of(target)]
    far = (block_of(target) + shards_of // 2) % shards_of
    return jnp.where((block_of(source) == first) | (block_of(source) == far), factor * drawn, drawn)


def block_levels(rng, extent, cuts, least, largest):
    loudness, own = 1.0, jax.random.fold_in(rng, 6)
    for position, blocks in cuts:
        draws = jnp.exp(jax.random.uniform(jax.random.fold_in(own, position), (blocks,), jnp.float32, least / len(cuts), largest / len(cuts)))
        loudness = loudness * jnp.repeat(draws, extent[position] // blocks).reshape([-1 if axis == position else 1 for axis in range(len(extent))])
    return loudness


def deal_out(own_key, own, number, rows, count, top, reach, skew):
    sequence = jax.random.permutation(own_key, count)
    heavy_load, common = portions_of(count, rows * top, reach, skew, True), portions_of(count, rows * top, reach, skew, False)
    places = jnp.arange(count)

    def named(sizes, rotation):
        used = int((sizes > 0).sum())
        fixed = max(1, used // 4)
        moved = fixed + (places - fixed + rotation * (used - fixed)) % max(1, count - fixed)
        return jnp.zeros((count,), jnp.int32).at[sequence[jnp.where(places < fixed, places, moved)]].set(jnp.asarray(sizes, jnp.int32))

    sizes = jnp.where(number % 4 == 0, named(heavy_load, number // 4), named(common, number - number // 4 - 1))
    mixed = jax.random.permutation(jax.random.fold_in(own, 3), count)
    donor, taker = mixed[0:count // 2 * 2:2], mixed[1:count // 2 * 2:2]
    slack = jnp.minimum(sizes[donor] - 1, reach - sizes[taker]) // 2
    slack = jnp.where((donor == sequence[0]) | (taker == sequence[0]) | (sizes[taker] == 0), 0, jnp.maximum(slack, 0))
    moved = jax.random.randint(jax.random.fold_in(own, 4), (count // 2,), 0, 1 << 20) % (slack + 1)
    sizes = sizes.at[donor].add(-moved).at[taker].add(moved)
    members = jnp.searchsorted(jnp.cumsum(sizes), jnp.arange(rows * top), side="right").astype(jnp.int32)
    listing = members.reshape(top, rows).T
    listing = listing[jax.random.permutation(jax.random.fold_in(own, 1), rows)]
    rotation = jax.random.randint(jax.random.fold_in(own, 2), (rows, 1), 0, top)
    return jnp.take_along_axis(listing, (jnp.arange(top)[None, :] + rotation) % top, axis=1)


def portions_of(number_of, total, most, skew, full):
    loads = [(1 << 20) // math.isqrt(standing ** skew) + 1 for standing in range(1, number_of + 1)]
    largest = most if full else min(most, max(-(-total // number_of), total * loads[0] // sum(loads)))
    least = 1 if total - largest >= number_of - 1 else 0
    given, spare = [largest] + [least] * (number_of - 1), total - largest - least * (number_of - 1)
    while spare > 0:
        movable = [i for i in range(1, number_of) if given[i] < largest] or [i for i in range(1, number_of) if given[i] < most]
        pool, remaining = sum([loads[i] for i in movable]), spare
        for i in movable:
            more = min(most - given[i], max(1, remaining * loads[i] // pool), spare)
            given[i] = given[i] + more
            spare = spare - more
    return np.array(given)


def bell_draw(own_key, extent, scale, limit, cuts=(), kind=jnp.bfloat16):
    level = block_levels(own_key, extent, cuts, -0.22, 0.18) if cuts else 1.0
    values = jax.random.normal(own_key, extent, jnp.float32) * scale * level
    return jnp.minimum(jnp.maximum(values, -limit), limit).astype(kind)


def gaussian_with(stream_key, shape, width, limit, cuts, heavy, kind=jnp.bfloat16):
    result = width * jax.random.normal(stream_key, shape, jnp.float32)
    if cuts:
        result = result * block_levels(stream_key, shape, cuts, -0.22, 0.18)
    return jnp.clip(strengthened(result, jax.random.fold_in(stream_key, 3), *heavy), -limit, limit).astype(kind)


def setup_inputs(seed: int = 0) -> dict:
    arg_keys = jax.random.split(jax.random.key(seed), 13)
    stream = bell_draw(arg_keys[0], (SEQUENCE_TOKENS, D), 2.5, 12.0, ((0, 8),))
    out_grad = gaussian_with(arg_keys[1], (SEQUENCE_TOKENS, D), 1.0, 6.0, ((0, 8),), (0, 1, 8, 2.0))
    routes_keys = jax.random.split(jax.random.fold_in(arg_keys[2], 1), SEQUENCE_TOKENS // TOK_DEV)
    routes_turns = jax.random.permutation(jax.random.fold_in(arg_keys[2], 3), SEQUENCE_TOKENS // TOK_DEV)
    routes = jax.vmap(lambda own, number: deal_out(jax.random.fold_in(arg_keys[2], 2), own, number, TOK_DEV, EXPERTS, 2, CAP, 1))(routes_keys, routes_turns).reshape((SEQUENCE_TOKENS, 2))
    route_weight = jnp.clip(jnp.exp(math.log(1.0) - 1.609438 * jax.random.uniform(arg_keys[3], (SEQUENCE_TOKENS, 2), jnp.float32) ** block_levels(arg_keys[3], (SEQUENCE_TOKENS, 2), ((0, 8),), -0.2, 0.2)), 0.2, 1.0)
    queries = bell_draw(arg_keys[4], (SEQUENCE_TOKENS, RETENTION_HEADS, KD), 1.0, 6.0, ((0, 8), (1, 4)))
    key_vectors = bell_draw(arg_keys[5], (SEQUENCE_TOKENS, RETENTION_HEADS, KD), 1.0, 6.0, ((0, 8), (1, 4)))
    value_vectors = bell_draw(arg_keys[6], (SEQUENCE_TOKENS, RETENTION_HEADS, VD), 1.0, 6.0, ((0, 8), (1, 4)))
    log_decay = draw_log_decay(jax.random.fold_in(arg_keys[12], 71), 0)
    out_proj = bell_draw(arg_keys[8], (D, HV), HV ** -0.5, 0.125, ((1, 4),))
    gate_weight = bell_draw(arg_keys[9], (EXPERTS, D, FF), D ** -0.5, 0.125, ((0, 8), (2, 4)))
    up_weight = bell_draw(arg_keys[10], (EXPERTS, D, FF), D ** -0.5, 0.125, ((0, 8), (2, 4)))
    down_weight = bell_draw(arg_keys[11], (EXPERTS, FF, D), FF ** -0.5, 0.1875, ((0, 8), (1, 4)))
    return dict(stream=stream, out_grad=out_grad, routes=routes, route_weight=route_weight, queries=queries, key_vectors=key_vectors, value_vectors=value_vectors, log_decay=log_decay, out_proj=out_proj, gate_weight=gate_weight, up_weight=up_weight, down_weight=down_weight)


CLAMP_LIMIT = 7.0
GATE_SLOPE = 1.702
EPSILON = 1e-06
TOP_PRECISION = lax.Precision.HIGHEST

def slot_numbers(route_block, expert_count):
    flat_ids = route_block.reshape(-1)
    onehot = (flat_ids[:, None] == jnp.arange(expert_count, dtype=jnp.int32)[None, :]).astype(jnp.int32)
    before = jnp.cumsum(onehot, axis=0) - onehot
    return (flat_ids, lax.optimization_barrier(jnp.sum(before * onehot, axis=1)).astype(jnp.int32))

def rotation_tables(start, count, key_width):
    frequency = 1.0 / 10000.0 ** jnp.linspace(0.0, 1.0, key_width // 2, dtype=jnp.float32)
    token_position = (start + jnp.arange(count, dtype=jnp.int32)).astype(jnp.float32)
    angles = token_position[:, None] * frequency[None, :]
    return (jnp.cos(angles), jnp.sin(angles))

def turn(field, cosines, sines):
    paired = field.reshape(field.shape[:-1] + (field.shape[-1] // 2, 2))
    even_part = paired[..., 0]
    odd_part = paired[..., 1]
    cos_rows = cosines[:, None, :]
    sin_rows = sines[:, None, :]
    turned = jnp.stack([even_part * cos_rows - odd_part * sin_rows, odd_part * cos_rows + even_part * sin_rows], axis=-1)
    return turned.reshape(field.shape)

def expert_pass(routed_rows, routed_grads, gate_w, up_w, down_w):
    gate_pre = jnp.dot(routed_rows, gate_w, preferred_element_type=jnp.float32)
    up_pre = jnp.dot(routed_rows, up_w, preferred_element_type=jnp.float32)
    gate_clip = jnp.minimum(gate_pre, CLAMP_LIMIT)
    up_clip = jnp.clip(up_pre, -CLAMP_LIMIT, CLAMP_LIMIT)
    sigmoid_gate = jax.nn.sigmoid(GATE_SLOPE * gate_clip)
    activated = (gate_clip * sigmoid_gate * (up_clip + 1.0)).astype(jnp.bfloat16)
    down_part = lax.dot_general(activated, routed_grads, (((0,), (0,)), ((), ())), preferred_element_type=jnp.float32)
    act_grad = lax.dot_general(routed_grads, down_w, (((1,), (1,)), ((), ())), preferred_element_type=jnp.float32)
    slope = sigmoid_gate + GATE_SLOPE * gate_clip * sigmoid_gate * (1.0 - sigmoid_gate)
    gate_pre_grad = jnp.where(gate_pre < CLAMP_LIMIT, act_grad * (up_clip + 1.0) * slope, 0.0).astype(jnp.bfloat16)
    up_pre_grad = jnp.where(jnp.abs(up_pre) < CLAMP_LIMIT, act_grad * gate_clip * sigmoid_gate, 0.0).astype(jnp.bfloat16)
    gate_part = lax.dot_general(routed_rows, gate_pre_grad, (((0,), (0,)), ((), ())), preferred_element_type=jnp.float32)
    up_part = lax.dot_general(routed_rows, up_pre_grad, (((0,), (0,)), ((), ())), preferred_element_type=jnp.float32)
    row_count = routed_rows.shape[0]
    group = gate_w.shape[1] // N_TP
    gate_groups = gate_pre_grad.reshape(row_count, N_TP, group).astype(jnp.float32)
    up_groups = up_pre_grad.reshape(row_count, N_TP, group).astype(jnp.float32)
    gate_w_groups = gate_w.reshape(gate_w.shape[0], N_TP, group).astype(jnp.float32)
    up_w_groups = up_w.reshape(up_w.shape[0], N_TP, group).astype(jnp.float32)
    partial_value = jnp.einsum('rtf,dtf->trd', gate_groups, gate_w_groups) + jnp.einsum('rtf,dtf->trd', up_groups, up_w_groups)
    rounded = lax.optimization_barrier(partial_value.astype(jnp.bfloat16))
    back_rows = lax.optimization_barrier(jnp.sum(rounded.astype(jnp.float32), axis=0)).astype(jnp.bfloat16)
    return (gate_part.astype(jnp.bfloat16), up_part.astype(jnp.bfloat16), down_part.astype(jnp.bfloat16), back_rows)

def prepare(query_block, key_block, value_block, decay_block, start):
    cosines, sines = rotation_tables(start, TOK_DEV, KD)
    query_rotated = turn(query_block.astype(jnp.float32), cosines, sines).transpose(1, 0, 2)
    key_rotated = (turn(key_block.astype(jnp.float32), cosines, sines) * KD ** (-0.5)).transpose(1, 0, 2)
    value_per_head = value_block.astype(jnp.float32).transpose(1, 0, 2)
    running_total = jnp.cumsum(decay_block, axis=0).T
    block_total = running_total[:, -1]
    causal = (jnp.arange(TOK_DEV)[:, None] >= jnp.arange(TOK_DEV)[None, :])[None]
    difference = running_total[:, :, None] - running_total[:, None, :]
    decay_mask = jnp.where(causal, jnp.exp(jnp.where(causal, difference, 0.0)), 0.0)
    return (query_rotated, key_rotated, value_per_head, running_total, block_total, decay_mask, cosines, sines)

def reference(stream, out_grad, routes, route_weight, queries, key_vectors, value_vectors, log_decay, out_proj, gate_weight, up_weight, down_weight):
    pair_count = 2 * TOK_DEV
    flat_ids, slot_ids = jax.vmap(lambda block_data: slot_numbers(block_data, EXPERTS))(routes.reshape(N_SP, TOK_DEV, 2))
    destination = flat_ids * CAP + slot_ids

    def place(target):
        return jnp.full((EXPERTS * CAP,), -1, jnp.int32).at[target].set(jnp.arange(pair_count, dtype=jnp.int32))
    source = jax.vmap(place)(destination)
    block_ids = jnp.arange(N_SP, dtype=jnp.int32)[:, None]
    present = source >= 0
    global_pair = jnp.where(present, block_ids * pair_count + source, 0).astype(jnp.int32)
    per_expert = global_pair.reshape(N_SP, EXPERTS, CAP).transpose(1, 0, 2).reshape(EXPERTS, N_SP * CAP)
    occupied = present.reshape(N_SP, EXPERTS, CAP).transpose(1, 0, 2).reshape(EXPERTS, N_SP * CAP)
    pair_grad = (route_weight[:, :, None] * out_grad[:, None, :].astype(jnp.float32)).astype(jnp.bfloat16)
    pair_grad = pair_grad.reshape(2 * SEQUENCE_TOKENS, D)
    zero_value = jnp.zeros((), jnp.bfloat16)

    def one_expert(expert_index):
        pair_ids = per_expert[expert_index]
        row_mask = occupied[expert_index][:, None]
        routed_rows = jnp.where(row_mask, jnp.take(stream, pair_ids // 2, axis=0), zero_value)
        routed_grads = jnp.where(row_mask, jnp.take(pair_grad, pair_ids, axis=0), zero_value)
        return expert_pass(routed_rows, routed_grads, gate_weight[expert_index], up_weight[expert_index], down_weight[expert_index])
    gate_grad, up_grad, down_grad, back_rows = lax.map(one_expert, jnp.arange(EXPERTS, dtype=jnp.int32))
    row_index = (flat_ids * (N_SP * CAP) + block_ids * CAP + slot_ids).astype(jnp.int32)
    per_pair = jnp.take(back_rows.reshape(EXPERTS * N_SP * CAP, D), row_index.reshape(-1), axis=0)
    per_pair = per_pair.reshape(SEQUENCE_TOKENS, 2, D).astype(jnp.float32)
    resid_grad = (out_grad.astype(jnp.float32) + per_pair[:, 0] + per_pair[:, 1]).astype(jnp.bfloat16)

    def to_blocks(array):
        return array.reshape((N_SP, TOK_DEV) + array.shape[1:])
    starts = jnp.arange(N_SP, dtype=jnp.int32) * TOK_DEV
    inputs = (to_blocks(queries), to_blocks(key_vectors), to_blocks(value_vectors), to_blocks(log_decay), starts)

    def forward(running_state, block_data):
        query_rotated, key_rotated, value_per_head, running_total, block_total, decay_mask, cosines, sines = prepare(*block_data)
        weights = jnp.einsum('hik,hjk->hij', query_rotated, key_rotated, precision=TOP_PRECISION) * decay_mask
        retained_output = jnp.einsum('hij,hjv->hiv', weights, value_per_head, precision=TOP_PRECISION)
        retained_output = retained_output + jnp.exp(running_total)[..., None] * jnp.einsum('dzr,drs->dzs', query_rotated, running_state, precision=TOP_PRECISION)
        remaining_decay = jnp.exp(block_total[:, None] - running_total)
        inner_state = jnp.einsum('wfs,wfi->wsi', key_rotated * remaining_decay[..., None], value_per_head, precision=TOP_PRECISION)
        new_state = jnp.exp(block_total)[:, None, None] * running_state + inner_state
        return (new_state, (retained_output, running_state))
    _, (retained_all, incoming_state) = lax.scan(forward, jnp.zeros((RETENTION_HEADS, KD, VD), jnp.float32), inputs)
    inverse_rms = lax.rsqrt(lax.optimization_barrier(jnp.mean(retained_all * retained_all, axis=-1, keepdims=True)) + EPSILON)
    normed = retained_all * inverse_rms
    normed_bf = normed.transpose(0, 2, 1, 3).reshape(SEQUENCE_TOKENS, HV).astype(jnp.bfloat16)
    proj_grad = lax.dot_general(resid_grad, normed_bf, (((0,), (0,)), ((), ())), preferred_element_type=jnp.float32)
    normed_grad = jnp.dot(resid_grad, out_proj, preferred_element_type=jnp.float32)
    normed_grad = normed_grad.reshape(N_SP, TOK_DEV, RETENTION_HEADS, VD).transpose(0, 2, 1, 3)
    retention_gradient = inverse_rms * (normed_grad - normed * lax.optimization_barrier(jnp.mean(normed_grad * normed, axis=-1, keepdims=True)))

    def backward(next_rows, block_data):
        block_inputs, running_state, gradient_tile = block_data
        query_rotated, key_rotated, value_per_head, running_total, block_total, decay_mask, cosines, sines = prepare(*block_inputs)
        per_head_decay = jnp.exp(running_total)
        remaining_decay = jnp.exp(block_total[:, None] - running_total)
        weights = jnp.einsum('hik,hjk->hij', query_rotated, key_rotated, precision=TOP_PRECISION) * decay_mask
        score_grad = jnp.einsum('hiv,hjv->hij', gradient_tile, value_per_head, precision=TOP_PRECISION) * decay_mask
        query_portion = jnp.einsum('hij,hjk->hik', score_grad, key_rotated, precision=TOP_PRECISION)
        query_portion = query_portion + per_head_decay[..., None] * jnp.einsum('bpl,btl->bpt', gradient_tile, running_state, precision=TOP_PRECISION)
        key_portion = jnp.einsum('hij,hik->hjk', score_grad, query_rotated, precision=TOP_PRECISION)
        key_portion = key_portion + remaining_decay[..., None] * jnp.einsum('uxn,ubn->uxb', value_per_head, next_rows, precision=TOP_PRECISION)
        value_portion = jnp.einsum('hij,hiv->hjv', weights, gradient_tile, precision=TOP_PRECISION)
        value_portion = value_portion + remaining_decay[..., None] * jnp.einsum('bui,bim->bum', key_rotated, next_rows, precision=TOP_PRECISION)
        inner_gradient = jnp.einsum('gwn,gwj->gnj', query_rotated * per_head_decay[..., None], gradient_tile, precision=TOP_PRECISION)
        earlier_grad = inner_gradient + jnp.exp(block_total)[:, None, None] * next_rows
        q_out = turn(query_portion.transpose(1, 0, 2), cosines, -sines).astype(jnp.bfloat16)
        k_out = (turn(key_portion.transpose(1, 0, 2), cosines, -sines) * KD ** (-0.5)).astype(jnp.bfloat16)
        v_out = value_portion.transpose(1, 0, 2).astype(jnp.bfloat16)
        return (earlier_grad, (q_out, k_out, v_out))
    _, (query_grad, key_grad, value_grad) = lax.scan(backward, jnp.zeros((RETENTION_HEADS, KD, VD), jnp.float32), (inputs, incoming_state, retention_gradient), reverse=True)
    query_grad = query_grad.reshape(SEQUENCE_TOKENS, RETENTION_HEADS, KD)
    key_grad = key_grad.reshape(SEQUENCE_TOKENS, RETENTION_HEADS, KD)
    value_grad = value_grad.reshape(SEQUENCE_TOKENS, RETENTION_HEADS, VD)
    return (gate_grad, up_grad, down_grad, proj_grad, query_grad, key_grad, value_grad)
```

```python
import functools

import jax
import jax.numpy as jnp
from jax import lax
from jax.experimental import pallas as pl
from jax.experimental.pallas import tpu as pltpu
from jax.sharding import PartitionSpec as P

CLAMP_LIMIT = 7.0
GATE_SLOPE = 1.702
EPSILON = 1e-06
F32 = jnp.float32
BF16 = jnp.bfloat16
MESH = pl.DeviceIdType.MESH


def any_specs(count):
    return [pl.BlockSpec(memory_space=pl.ANY)] * count


def vmem_specs(count):
    return [pl.BlockSpec(memory_space=pltpu.VMEM)] * count


def tp_partners(c, n_tp):
    far = lax.rem(c + n_tp // 2, n_tp)
    near = c + 1 - 2 * lax.rem(c, 2)
    return far, near


def greet(n_sp, me, c, sp_peers, tp_peers):
    barrier = pltpu.get_barrier_semaphore()
    count = 0
    if sp_peers:
        for k in range(1, n_sp):
            pl.semaphore_signal(
                barrier, inc=1, device_id=(lax.rem(me + k, n_sp), c), device_id_type=MESH
            )
            count += 1
    for t in tp_peers:
        pl.semaphore_signal(barrier, inc=1, device_id=(me, t), device_id_type=MESH)
        count += 1
    pl.semaphore_wait(barrier, count)


def push(src, dst, send_sem, recv_sem, device):
    return pltpu.make_async_remote_copy(
        src_ref=src,
        dst_ref=dst,
        send_sem=send_sem,
        recv_sem=recv_sem,
        device_id=device,
        device_id_type=MESH,
    )


def dispatch_kernel(
    n_sp, n_tp, q, rows, grads, tot, rows_out, grads_out, tot_out,
    own_sem, ssem, rsem, xssem, xrsem, dssem, drsem, essem, ersem, tssem, trsem,
):
    me = lax.axis_index("sp")
    c = lax.axis_index("tp")
    far, near = tp_partners(c, n_tp)
    greet(n_sp, me, c, True, (far, near))
    arrays = ((rows, rows_out), (grads, grads_out))

    def cols(quarter):
        return pl.ds(pl.multiple_of(quarter * q, 128), q)

    waits = []
    for k in range(1, n_sp):
        peer = lax.rem(me + k, n_sp)
        cp = push(tot, tot_out.at[me], tssem.at[k], trsem.at[k], (peer, c))
        cp.start()
        waits.append(cp)
        for a, (src, out) in enumerate(arrays):
            cp = push(
                src.at[peer], out.at[me, :, cols(c)], ssem.at[a, k], rsem.at[a, k], (peer, c)
            )
            cp.start()
            waits.append(cp)
    local = [pltpu.make_async_copy(tot, tot_out.at[me], own_sem.at[2])]
    for a, (src, out) in enumerate(arrays):
        local.append(pltpu.make_async_copy(src.at[me], out.at[me, :, cols(c)], own_sem.at[a]))
    for cp in local:
        cp.start()
    sent = []
    last = []

    def relay(k):
        source = lax.rem(me + n_sp - k, n_sp)
        for a, (src, out) in enumerate(arrays):
            spot = out.at[source, :, cols(far)]
            push(spot, spot, xssem.at[a, k], xrsem.at[a, k], (me, far)).wait_recv()
            cp = push(spot, spot, essem.at[a, k], ersem.at[a, k], (me, near))
            cp.start()
            sent.append(cp)
            last.append((out, source, a, k))

    for k in range(n_sp):
        source = lax.rem(me + n_sp - k, n_sp)
        for a, (src, out) in enumerate(arrays):
            spot = out.at[source, :, cols(c)]
            if k == 0:
                origin = src.at[me]
            else:
                push(spot, spot, ssem.at[a, k], rsem.at[a, k], (me, far)).wait_recv()
                origin = spot
            for sems, device in (((xssem, xrsem), far), ((dssem, drsem), near)):
                cp = push(origin, spot, sems[0].at[a, k], sems[1].at[a, k], (me, device))
                cp.start()
                sent.append(cp)
        if k >= 1:
            relay(k - 1)
    relay(n_sp - 1)
    near_far = lax.rem(near + n_tp // 2, n_tp)
    for out, source, a, k in last:
        spot = out.at[source, :, cols(near)]
        push(spot, spot, dssem.at[a, k], drsem.at[a, k], (me, near)).wait_recv()
        spot = out.at[source, :, cols(near_far)]
        push(spot, spot, essem.at[a, k], ersem.at[a, k], (me, near)).wait_recv()
    for k in range(1, n_sp):
        source = lax.rem(me + n_sp - k, n_sp)
        spot = tot_out.at[source]
        push(spot, spot, tssem.at[k], trsem.at[k], (me, far)).wait_recv()
    for cp in waits + sent:
        cp.wait_send()
    for cp in local:
        cp.wait()


def dispatch(rows, grads, tot, n_tp):
    n_sp, cap, q = rows.shape
    full = jax.ShapeDtypeStruct((n_sp, cap, q * n_tp), rows.dtype)
    dma = pltpu.SemaphoreType.DMA
    return pl.pallas_call(
        functools.partial(dispatch_kernel, n_sp, n_tp, q),
        out_shape=(full, full, jax.ShapeDtypeStruct((n_sp,) + tot.shape, tot.dtype)),
        in_specs=any_specs(3),
        out_specs=tuple(any_specs(3)),
        scratch_shapes=[dma((3,))] + [dma((2, n_sp))] * 8 + [dma((n_sp,))] * 2,
        compiler_params=pltpu.CompilerParams(collective_id=0, has_side_effects=True),
        name="dispatch",
    )(rows, grads, tot)


def return_kernel(
    n_sp, n_tp, q, back, comb, og, resid,
    part, xbuf, xrecv, sendbuf, ret, resq,
    pssem, prsem, xssem, xrsem, ssem, rsem, gssem, grsem,
):
    me = lax.axis_index("sp")
    c = lax.axis_index("tp")
    far, near = tp_partners(c, n_tp)
    near_far = lax.rem(near + n_tp // 2, n_tp)
    greet(n_sp, me, c, True, (far, near))

    def cols(quarter):
        return pl.ds(pl.multiple_of(quarter * q, 128), q)

    order = list(range(1, n_sp)) + [0]
    waits = []
    for k in order:
        i = lax.rem(me + k, n_sp)
        for b, quarter in enumerate((near_far, near)):
            cp = push(
                back.at[i, :, cols(quarter)], part.at[b, k], pssem.at[b, k], prsem.at[b, k],
                (me, near),
            )
            cp.start()
            waits.append(cp)

    def to_far(k):
        cp = push(xbuf.at[k], xrecv.at[k], xssem.at[k], xrsem.at[k], (me, far))
        cp.start()
        waits.append(cp)

    def to_home(k):
        cp = push(
            sendbuf.at[k], ret.at[me], ssem.at[k], rsem.at[k], (lax.rem(me + k, n_sp), c)
        )
        cp.start()
        waits.append(cp)

    def first(k):
        i = lax.rem(me + k, n_sp)
        push(xbuf.at[k], part.at[0, k], pssem.at[0, k], prsem.at[0, k], (me, near)).wait_recv()
        xbuf[k] = (back[i, :, cols(far)].astype(F32) + part[0, k].astype(F32)).astype(BF16)

    def second(k):
        i = lax.rem(me + k, n_sp)
        push(xbuf.at[k], part.at[1, k], pssem.at[1, k], prsem.at[1, k], (me, near)).wait_recv()
        push(xbuf.at[k], xrecv.at[k], xssem.at[k], xrsem.at[k], (me, far)).wait_recv()
        total = (
            back[i, :, cols(c)].astype(F32) + part[1, k].astype(F32) + xrecv[k].astype(F32)
        ).astype(BF16)
        if k == 0:
            ret[me] = total
        else:
            sendbuf[k] = total

    lag = 2
    for n in range(n_sp + lag + 1):
        if n < n_sp:
            first(order[n])
        if 1 <= n <= n_sp:
            to_far(order[n - 1])
        if lag <= n < n_sp + lag:
            second(order[n - lag])
        if n >= lag + 1 and order[n - lag - 1] != 0:
            to_home(order[n - lag - 1])
    for k in range(1, n_sp):
        source = lax.rem(me + n_sp - k, n_sp)
        push(sendbuf.at[k], ret.at[source], ssem.at[k], rsem.at[k], (me, far)).wait_recv()
    cap = back.shape[1]
    returned = ret[...].astype(F32).reshape(n_sp * cap, q).astype(BF16)
    resq[...] = (
        og[...].astype(F32) + jnp.dot(comb[...], returned, preferred_element_type=F32)
    ).astype(BF16)
    mine = resid.at[:, cols(c)]
    own = pltpu.make_async_copy(resq, mine, gssem.at[3])
    own.start()
    for s, device in enumerate((far, near)):
        cp = push(resq, mine, gssem.at[s], grsem.at[s], (me, device))
        cp.start()
        waits.append(cp)
    spot = resid.at[:, cols(far)]
    push(resq, spot, gssem.at[0], grsem.at[0], (me, far)).wait_recv()
    cp = push(spot, spot, gssem.at[2], grsem.at[2], (me, near))
    cp.start()
    waits.append(cp)
    push(resq, resid.at[:, cols(near)], gssem.at[1], grsem.at[1], (me, near)).wait_recv()
    push(resq, resid.at[:, cols(near_far)], gssem.at[2], grsem.at[2], (me, near)).wait_recv()
    own.wait()
    for cp in waits:
        cp.wait_send()


def give_back(back, comb, og_q, n_tp):
    n_sp, cap, width = back.shape
    q = width // n_tp
    tokens = og_q.shape[0]
    dma = pltpu.SemaphoreType.DMA
    block = pltpu.VMEM((n_sp, cap, q), BF16)
    return pl.pallas_call(
        functools.partial(return_kernel, n_sp, n_tp, q),
        out_shape=jax.ShapeDtypeStruct((tokens, width), BF16),
        in_specs=vmem_specs(3),
        out_specs=pl.BlockSpec(memory_space=pl.ANY),
        scratch_shapes=[pltpu.VMEM((2, n_sp, cap, q), BF16)]
        + [block] * 4
        + [pltpu.VMEM((tokens, q), BF16)]
        + [dma((2, n_sp))] * 2
        + [dma((n_sp,))] * 4
        + [dma((4,)), dma((3,))],
        compiler_params=pltpu.CompilerParams(collective_id=1, has_side_effects=True),
        name="give_back",
    )(back, comb, og_q)


def swap_kernel(n_sp, w, resid, state, cols_out, states, own_sem, ssem, rsem):
    me = lax.axis_index("sp")
    c = lax.axis_index("tp")
    greet(n_sp, me, c, True, ())

    def part(index):
        if len(resid.shape) == 3:
            return resid.at[index]
        return resid.at[:, pl.ds(pl.multiple_of(index * w, 128), w)]

    waits = []
    for k in range(1, n_sp):
        peer = lax.rem(me + k, n_sp)
        for a, (src, out) in enumerate(((state, states), (part(peer), cols_out))):
            cp = push(src, out.at[me], ssem.at[a, k], rsem.at[a, k], (peer, c))
            cp.start()
            waits.append(cp)
    local = [
        pltpu.make_async_copy(part(me), cols_out.at[me], own_sem.at[0]),
        pltpu.make_async_copy(state, states.at[me], own_sem.at[1]),
    ]
    for cp in local:
        cp.start()
    for k in range(1, n_sp):
        source = lax.rem(me + n_sp - k, n_sp)
        for a, out in enumerate((states, cols_out)):
            spot = out.at[source]
            push(spot, spot, ssem.at[a, k], rsem.at[a, k], (source, c)).wait_recv()
    for cp in waits:
        cp.wait_send()
    for cp in local:
        cp.wait()


def swap(resid, state, n_sp):
    tokens, width = resid.shape
    w = width // n_sp
    if w % 128:
        resid = resid.reshape(tokens, n_sp, w).transpose(1, 0, 2)
    dma = pltpu.SemaphoreType.DMA
    return pl.pallas_call(
        functools.partial(swap_kernel, n_sp, w),
        out_shape=(
            jax.ShapeDtypeStruct((n_sp, tokens, w), BF16),
            jax.ShapeDtypeStruct((n_sp,) + state.shape, BF16),
        ),
        in_specs=any_specs(2),
        out_specs=tuple(any_specs(2)),
        scratch_shapes=[dma((2,)), dma((2, n_sp)), dma((2, n_sp))],
        compiler_params=pltpu.CompilerParams(collective_id=2, has_side_effects=True),
        name="swap",
    )(resid, state)


def rotation_tables(start, count, key_width):
    frequency = 1.0 / 10000.0 ** jnp.linspace(0.0, 1.0, key_width // 2, dtype=F32)
    frequency = jnp.repeat(frequency, 2)
    token_position = (start + jnp.arange(count, dtype=jnp.int32)).astype(F32)
    angles = token_position[:, None] * frequency[None, :]
    return (jnp.cos(angles)[None], jnp.sin(angles)[None])


def swap_matrix(key_width):
    row = jnp.arange(key_width)[:, None]
    col = jnp.arange(key_width)[None, :]
    up = (col == row + 1) & (row % 2 == 0)
    down = (col == row - 1) & (row % 2 == 1)
    return (up.astype(F32) - down.astype(F32)).astype(BF16)


def turn(field, cosines, sines, matrix):
    turned = jnp.einsum("htk,kl->htl", field.astype(BF16), matrix, preferred_element_type=F32)
    return field.astype(F32) * cosines + turned * sines


def ein(spec, a, b):
    return jnp.einsum(spec, a.astype(BF16), b.astype(BF16), preferred_element_type=F32)


def fine(spec, a, b):
    return jnp.einsum(spec, a.astype(F32), b.astype(F32), precision=lax.Precision.HIGHEST)


def mm(a, b, da, db):
    return lax.dot_general(a, b, (((da,), (db,)), ((), ())), preferred_element_type=F32)


def expert_local(routed_rows, routed_grads, gate_w, up_w, down_w):
    gate_pre = mm(routed_rows, gate_w, 1, 0)
    up_pre = mm(routed_rows, up_w, 1, 0)
    gate_clip = jnp.minimum(gate_pre, CLAMP_LIMIT)
    up_clip = jnp.clip(up_pre, -CLAMP_LIMIT, CLAMP_LIMIT)
    sigmoid_gate = jax.nn.sigmoid(GATE_SLOPE * gate_clip)
    activated = (gate_clip * sigmoid_gate * (up_clip + 1.0)).astype(BF16)
    down_part = mm(activated, routed_grads, 0, 0)
    act_grad = mm(routed_grads, down_w, 1, 1)
    slope = sigmoid_gate + GATE_SLOPE * gate_clip * sigmoid_gate * (1.0 - sigmoid_gate)
    gate_pre_grad = jnp.where(
        gate_pre < CLAMP_LIMIT, act_grad * (up_clip + 1.0) * slope, 0.0
    ).astype(BF16)
    up_pre_grad = jnp.where(
        jnp.abs(up_pre) < CLAMP_LIMIT, act_grad * gate_clip * sigmoid_gate, 0.0
    ).astype(BF16)
    gate_part = mm(routed_rows, gate_pre_grad, 0, 0)
    up_part = mm(routed_rows, up_pre_grad, 0, 0)
    back_rows = mm(gate_pre_grad, gate_w, 1, 1) + mm(up_pre_grad, up_w, 1, 1)
    return (
        gate_part.astype(BF16),
        up_part.astype(BF16),
        down_part.astype(BF16),
        back_rows.astype(BF16),
    )


def per_device(
    stream, out_grad, routes, route_weight, queries, key_vectors, value_vectors, log_decay,
    out_proj, gate_weight, up_weight, down_weight,
):
    n_sp = lax.axis_size("sp")
    n_tp = lax.axis_size("tp")
    me = lax.axis_index("sp")
    tokens, width = stream.shape
    capacity = 4 * tokens // n_sp
    slots = n_sp * capacity
    quarter = width // n_tp
    heads = queries.shape[1]
    key_width = queries.shape[2]
    value_width = value_vectors.shape[2]

    ids = jnp.arange(n_sp, dtype=jnp.int32)
    chosen = routes[:, :, None] == ids[None, None, :]
    counts = jnp.sum(chosen.astype(F32), axis=1).astype(BF16)
    place = jnp.arange(tokens)
    lower = (place[:, None] > place[None, :]).astype(BF16)
    before = jnp.dot(lower, counts, preferred_element_type=F32)
    slot = jnp.sum(jnp.where(chosen, before[:, None, :], 0.0), axis=2).astype(jnp.int32)
    target = routes * capacity + slot
    spots = jnp.arange(slots, dtype=jnp.int32)
    hit = target.T[:, None, :] == spots[None, :, None]
    pick = (hit[0] | hit[1]).astype(BF16)
    weight = jnp.sum(
        jnp.where(hit[0], route_weight[None, :, 0], 0.0)
        + jnp.where(hit[1], route_weight[None, :, 1], 0.0),
        axis=1,
    )
    comb = ((target[:, :1] == spots[None, :]) | (target[:, 1:] == spots[None, :])).astype(BF16)
    col_start = lax.axis_index("tp") * quarter
    stream_q = lax.dynamic_slice_in_dim(stream, col_start, quarter, 1)
    og_q = lax.dynamic_slice_in_dim(out_grad, col_start, quarter, 1)
    send_rows = jnp.dot(pick, stream_q, preferred_element_type=F32).astype(BF16)
    send_grads = (
        weight[:, None] * jnp.dot(pick, og_q, preferred_element_type=F32)
    ).astype(BF16)

    running = jnp.cumsum(log_decay, axis=0).T
    block_total = running[:, -1]
    tot = jnp.broadcast_to(jnp.pad(block_total, (0, 128 - heads))[None, :], (8, 128))
    rows, grads, tots = dispatch(
        send_rows.reshape(n_sp, capacity, quarter),
        send_grads.reshape(n_sp, capacity, quarter),
        tot,
        n_tp,
    )

    matrix = swap_matrix(key_width)
    cosines, sines = rotation_tables(me * tokens, tokens, key_width)
    scale = key_width ** (-0.5)
    query_rot = turn(queries.transpose(1, 0, 2), cosines, sines, matrix)
    key_rot = turn(key_vectors.transpose(1, 0, 2), cosines, sines, matrix) * scale
    values = value_vectors.transpose(1, 0, 2)
    causal = (place[:, None] >= place[None, :])[None]
    difference = running[:, :, None] - running[:, None, :]
    mask = jnp.where(causal, jnp.exp(jnp.where(causal, difference, 0.0)), 0.0)
    decay = jnp.exp(running)[..., None]
    remaining = jnp.exp(block_total[:, None] - running)[..., None]
    inner = ein("wfs,wfi->wsi", key_rot * remaining, values).astype(BF16)
    inner_all = lax.all_gather(inner, "sp")
    key_bf = key_rot.astype(BF16)
    query_bf = query_rot.astype(BF16)
    weights = fine("hik,hjk->hij", query_rot, key_rot) * mask
    retained_local = fine("hij,hjv->hiv", weights, values)

    gate_part, up_part, down_part, back_rows = expert_local(
        rows.reshape(slots, width),
        grads.reshape(slots, width),
        gate_weight[0],
        up_weight[0],
        down_weight[0],
    )
    totals = tots[:, 0, :heads]
    sums = jnp.cumsum(totals, axis=0)
    sum_before = jnp.sum(jnp.where((ids < me)[:, None], totals, 0.0), axis=0)
    sum_through = sum_before + block_total
    past = jnp.where((ids < me)[:, None], sum_before[None] - sums, 0.0)
    past = jnp.where((ids < me)[:, None], jnp.exp(past), 0.0)
    coming = jnp.where((ids > me)[:, None], sums - totals - sum_through[None], 0.0)
    coming = jnp.where((ids > me)[:, None], jnp.exp(coming), 0.0)
    incoming = jnp.sum(inner_all.astype(F32) * past[:, :, None, None], axis=0)
    retained = retained_local + decay * fine("dzr,drs->dzs", query_rot, incoming)
    inverse_rms = lax.rsqrt(jnp.mean(retained * retained, axis=-1, keepdims=True) + EPSILON)
    normed = retained * inverse_rms
    normed_bf = normed.transpose(1, 0, 2).reshape(tokens, heads * value_width).astype(BF16)
    normed_all = lax.all_gather(normed_bf, "sp", axis=0, tiled=True)

    resid = give_back(back_rows.reshape(n_sp, capacity, width), comb, og_q, n_tp)
    normed_grad = jnp.dot(resid, out_proj, preferred_element_type=F32)
    normed_grad = normed_grad.reshape(tokens, heads, value_width).transpose(1, 0, 2)
    grad = inverse_rms * (
        normed_grad - normed * jnp.mean(normed_grad * normed, axis=-1, keepdims=True)
    )
    grad_bf = grad.astype(BF16)
    inner_grad = ein("gwn,gwj->gnj", query_rot * decay, grad_bf).astype(BF16)
    resid_cols, grads_all = swap(resid, inner_grad, n_sp)
    future = jnp.sum(grads_all.astype(F32) * coming[:, :, None, None], axis=0).astype(BF16)
    score = fine("hiv,hjv->hij", grad, values) * mask
    query_portion = ein("hij,hjk->hik", score, key_bf) + decay * fine(
        "bpl,btl->bpt", grad, incoming
    )
    key_portion = ein("hij,hik->hjk", score, query_bf) + remaining * ein(
        "uxn,ubn->uxb", values, future
    )
    value_portion = ein("hij,hiv->hjv", weights, grad_bf) + remaining * ein(
        "bui,bim->bum", key_bf, future
    )
    query_grad = turn(query_portion, cosines, -sines, matrix).astype(BF16).transpose(1, 0, 2)
    key_grad = (
        (turn(key_portion, cosines, -sines, matrix) * scale).astype(BF16).transpose(1, 0, 2)
    )
    value_grad = value_portion.astype(BF16).transpose(1, 0, 2)
    proj_grad = mm(resid_cols.reshape(n_sp * tokens, -1), normed_all, 0, 0)
    return (
        gate_part[None],
        up_part[None],
        down_part[None],
        proj_grad,
        query_grad,
        key_grad,
        value_grad,
    )


def solution(mesh):
    in_specs = (
        P("sp", None),
        P("sp", None),
        P("sp", None),
        P("sp", None),
        P("sp", "tp", None),
        P("sp", "tp", None),
        P("sp", "tp", None),
        P("sp", "tp"),
        P(None, "tp"),
        P("sp", None, "tp"),
        P("sp", None, "tp"),
        P("sp", "tp", None),
    )
    out_specs = (
        P("sp", None, "tp"),
        P("sp", None, "tp"),
        P("sp", "tp", None),
        P("sp", "tp"),
        P("sp", "tp", None),
        P("sp", "tp", None),
        P("sp", "tp", None),
    )
    return jax.shard_map(
        per_device, mesh=mesh, in_specs=in_specs, out_specs=out_specs, check_vma=False
    )
```

```python
import functools

import jax
import jax.numpy as jnp
from jax import lax
from jax.experimental import pallas as pl
from jax.experimental.pallas import tpu as pltpu
from jax.sharding import PartitionSpec as P

CLAMP_LIMIT = 7.0
GATE_SLOPE = 1.702
EPSILON = 1e-06
F32 = jnp.float32
BF16 = jnp.bfloat16
MESH = pl.DeviceIdType.MESH


def any_specs(count):
    return [pl.BlockSpec(memory_space=pl.ANY)] * count


def vmem_specs(count):
    return [pl.BlockSpec(memory_space=pltpu.VMEM)] * count


def tp_partners(c, n_tp):
    far = lax.rem(c + n_tp // 2, n_tp)
    near = c + 1 - 2 * lax.rem(c, 2)
    return far, near


def greet(n_sp, me, c, sp_peers, tp_peers):
    barrier = pltpu.get_barrier_semaphore()
    count = 0
    if sp_peers:
        for k in range(1, n_sp):
            pl.semaphore_signal(
                barrier, inc=1, device_id=(lax.rem(me + k, n_sp), c), device_id_type=MESH
            )
            count += 1
    for t in tp_peers:
        pl.semaphore_signal(barrier, inc=1, device_id=(me, t), device_id_type=MESH)
        count += 1
    pl.semaphore_wait(barrier, count)


def push(src, dst, send_sem, recv_sem, device):
    return pltpu.make_async_remote_copy(
        src_ref=src,
        dst_ref=dst,
        send_sem=send_sem,
        recv_sem=recv_sem,
        device_id=device,
        device_id_type=MESH,
    )


class Chain:
    def __init__(self, src, out, n_sp, me, c, sems, ways):
        self.src, self.out, self.me, self.c = src, out, me, c
        self.pairs, self.ways = n_sp // 2, ways
        self.pair = me // 2
        self.other = me + 1 - 2 * lax.rem(me, 2)
        self.zs, self.zr, self.ys, self.yr, self.own_sem = sems

    def has(self, d, way):
        return self.pair >= d if way == 0 else self.pair + d < self.pairs

    def room(self, way):
        return self.pair + 1 < self.pairs if way == 0 else self.pair >= 1

    def spot(self, base, d, way):
        return self.out.at[base - 2 * d if way == 0 else base + 2 * d]

    def along(self, d, way):
        spot = self.spot(self.me, d, way)
        return push(
            self.src if d == 0 else spot, spot, self.zs.at[way, d], self.zr.at[way, d + 1],
            (self.me + 2 if way == 0 else self.me - 2, self.c),
        )

    def across(self, d, way):
        spot = self.spot(self.me, d, way)
        return push(
            self.src if d == 0 else spot, spot, self.ys.at[way, d], self.yr.at[way, d],
            (self.other, self.c),
        )

    def own(self):
        return pltpu.make_async_copy(self.src, self.out.at[self.me], self.own_sem.at[0])

    def each(self, d, act):
        for way in self.ways:

            @pl.when(self.has(d, way))
            def _():
                if d < self.pairs - 1:

                    @pl.when(self.room(way))
                    def _():
                        act(self.along(d, way))

                if d > 0 or way == self.ways[0]:
                    act(self.across(d, way))

    def start(self):
        self.own().start()
        self.each(0, lambda cp: cp.start())

    def step(self, d):
        for way in self.ways:

            @pl.when(self.has(d, way))
            def _():
                spot = self.spot(self.me, d, way)
                push(
                    spot, spot, self.zs.at[way, d], self.zr.at[way, d], (self.other, self.c)
                ).wait_recv()

        self.each(d, lambda cp: cp.start())

    def finish(self):
        for d in range(self.pairs):
            for way in self.ways:
                if d == 0 and way != self.ways[0]:
                    continue

                @pl.when(self.has(d, way))
                def _():
                    spot = self.spot(self.other, d, way)
                    push(
                        spot, spot, self.ys.at[way, d], self.yr.at[way, d], (self.other, self.c)
                    ).wait_recv()

            self.each(d, lambda cp: cp.wait_send())
        self.own().wait()


def chain_sems(n_sp):
    dma = pltpu.SemaphoreType.DMA
    return [dma((2, n_sp // 2))] * 4 + [dma((1,))]


def dispatch_kernel(
    n_sp, n_tp, q, rows, grads, tot, state, rows_out, grads_out, tot_out, states,
    own_sem, ssem, rsem, xssem, xrsem, dssem, drsem, essem, ersem, tssem, trsem, *chain_sem,
):
    me = lax.axis_index("sp")
    c = lax.axis_index("tp")
    far, near = tp_partners(c, n_tp)
    greet(n_sp, me, c, True, (far, near))
    arrays = ((rows, rows_out), (grads, grads_out))

    def cols(quarter):
        return pl.ds(pl.multiple_of(quarter * q, 128), q)

    chain = Chain(state, states, n_sp, me, c, chain_sem, (0,))
    chain.start()
    waits = []
    for k in range(1, n_sp):
        peer = lax.rem(me + k, n_sp)
        cp = push(tot, tot_out.at[me], tssem.at[k], trsem.at[k], (peer, c))
        cp.start()
        waits.append(cp)
        for a, (src, out) in enumerate(arrays):
            cp = push(
                src.at[peer], out.at[me, :, cols(c)], ssem.at[a, k], rsem.at[a, k], (peer, c)
            )
            cp.start()
            waits.append(cp)
    local = [pltpu.make_async_copy(tot, tot_out.at[me], own_sem.at[2])]
    for a, (src, out) in enumerate(arrays):
        local.append(pltpu.make_async_copy(src.at[me], out.at[me, :, cols(c)], own_sem.at[a]))
    for cp in local:
        cp.start()
    sent = []
    last = []

    def relay(k):
        source = lax.rem(me + n_sp - k, n_sp)
        for a, (src, out) in enumerate(arrays):
            spot = out.at[source, :, cols(far)]
            push(spot, spot, xssem.at[a, k], xrsem.at[a, k], (me, far)).wait_recv()
            cp = push(spot, spot, essem.at[a, k], ersem.at[a, k], (me, near))
            cp.start()
            sent.append(cp)
            last.append((out, source, a, k))

    for k in range(n_sp):
        source = lax.rem(me + n_sp - k, n_sp)
        for a, (src, out) in enumerate(arrays):
            spot = out.at[source, :, cols(c)]
            if k == 0:
                origin = src.at[me]
            else:
                push(spot, spot, ssem.at[a, k], rsem.at[a, k], (me, far)).wait_recv()
                origin = spot
            for sems, device in (((xssem, xrsem), far), ((dssem, drsem), near)):
                cp = push(origin, spot, sems[0].at[a, k], sems[1].at[a, k], (me, device))
                cp.start()
                sent.append(cp)
        if k >= 1:
            relay(k - 1)
        if k and k % 2 == 0:
            chain.step(k // 2)
    relay(n_sp - 1)
    near_far = lax.rem(near + n_tp // 2, n_tp)
    for out, source, a, k in last:
        spot = out.at[source, :, cols(near)]
        push(spot, spot, dssem.at[a, k], drsem.at[a, k], (me, near)).wait_recv()
        spot = out.at[source, :, cols(near_far)]
        push(spot, spot, essem.at[a, k], ersem.at[a, k], (me, near)).wait_recv()
    for k in range(1, n_sp):
        source = lax.rem(me + n_sp - k, n_sp)
        spot = tot_out.at[source]
        push(spot, spot, tssem.at[k], trsem.at[k], (me, far)).wait_recv()
    for cp in waits + sent:
        cp.wait_send()
    for cp in local:
        cp.wait()
    chain.finish()


def dispatch(rows, grads, tot, state, n_tp):
    n_sp, cap, q = rows.shape
    full = jax.ShapeDtypeStruct((n_sp, cap, q * n_tp), rows.dtype)
    dma = pltpu.SemaphoreType.DMA
    return pl.pallas_call(
        functools.partial(dispatch_kernel, n_sp, n_tp, q),
        out_shape=(
            full,
            full,
            jax.ShapeDtypeStruct((n_sp,) + tot.shape, tot.dtype),
            jax.ShapeDtypeStruct((n_sp,) + state.shape, state.dtype),
        ),
        in_specs=any_specs(4),
        out_specs=tuple(any_specs(4)),
        scratch_shapes=[dma((3,))] + [dma((2, n_sp))] * 8 + [dma((n_sp,))] * 2 + chain_sems(n_sp),
        compiler_params=pltpu.CompilerParams(collective_id=0, has_side_effects=True),
        name="dispatch",
    )(rows, grads, tot, state)


def return_kernel(
    n_sp, n_tp, q, back, comb, og, normed, resid, normed_all,
    part, xbuf, xrecv, sendbuf, ret, resq,
    pssem, prsem, xssem, xrsem, ssem, rsem, gssem, grsem, *chain_sem,
):
    me = lax.axis_index("sp")
    c = lax.axis_index("tp")
    far, near = tp_partners(c, n_tp)
    near_far = lax.rem(near + n_tp // 2, n_tp)
    greet(n_sp, me, c, True, (far, near))

    def cols(quarter):
        return pl.ds(pl.multiple_of(quarter * q, 128), q)

    order = list(range(1, n_sp)) + [0]
    waits = []
    for k in order:
        i = lax.rem(me + k, n_sp)
        for b, quarter in enumerate((near_far, near)):
            cp = push(
                back.at[i, :, cols(quarter)], part.at[b, k], pssem.at[b, k], prsem.at[b, k],
                (me, near),
            )
            cp.start()
            waits.append(cp)
    chain = Chain(normed, normed_all, n_sp, me, c, chain_sem, (0, 1))
    chain.start()

    def to_far(k):
        cp = push(xbuf.at[k], xrecv.at[k], xssem.at[k], xrsem.at[k], (me, far))
        cp.start()
        waits.append(cp)

    def to_home(k):
        cp = push(
            sendbuf.at[k], ret.at[me], ssem.at[k], rsem.at[k], (lax.rem(me + k, n_sp), c)
        )
        cp.start()
        waits.append(cp)

    def first(k):
        i = lax.rem(me + k, n_sp)
        push(xbuf.at[k], part.at[0, k], pssem.at[0, k], prsem.at[0, k], (me, near)).wait_recv()
        xbuf[k] = (back[i, :, cols(far)].astype(F32) + part[0, k].astype(F32)).astype(BF16)

    def second(k):
        i = lax.rem(me + k, n_sp)
        push(xbuf.at[k], part.at[1, k], pssem.at[1, k], prsem.at[1, k], (me, near)).wait_recv()
        push(xbuf.at[k], xrecv.at[k], xssem.at[k], xrsem.at[k], (me, far)).wait_recv()
        total = (
            back[i, :, cols(c)].astype(F32) + part[1, k].astype(F32) + xrecv[k].astype(F32)
        ).astype(BF16)
        if k == 0:
            ret[me] = total
        else:
            sendbuf[k] = total

    lag = 2
    for n in range(n_sp + lag + 1):
        if n < n_sp:
            first(order[n])
        if 1 <= n <= n_sp:
            to_far(order[n - 1])
        if lag <= n < n_sp + lag:
            second(order[n - lag])
        if n >= lag + 1 and order[n - lag - 1] != 0:
            to_home(order[n - lag - 1])
        if n and n % 2 == 0 and n < n_sp:
            chain.step(n // 2)
    for k in range(1, n_sp):
        source = lax.rem(me + n_sp - k, n_sp)
        push(sendbuf.at[k], ret.at[source], ssem.at[k], rsem.at[k], (me, far)).wait_recv()
    cap = back.shape[1]
    returned = ret[...].astype(F32).reshape(n_sp * cap, q).astype(BF16)
    resq[...] = (
        og[...].astype(F32) + jnp.dot(comb[...], returned, preferred_element_type=F32)
    ).astype(BF16)
    mine = resid.at[:, cols(c)]
    own = pltpu.make_async_copy(resq, mine, gssem.at[3])
    own.start()
    for s, device in enumerate((far, near)):
        cp = push(resq, mine, gssem.at[s], grsem.at[s], (me, device))
        cp.start()
        waits.append(cp)
    spot = resid.at[:, cols(far)]
    push(resq, spot, gssem.at[0], grsem.at[0], (me, far)).wait_recv()
    cp = push(spot, spot, gssem.at[2], grsem.at[2], (me, near))
    cp.start()
    waits.append(cp)
    push(resq, resid.at[:, cols(near)], gssem.at[1], grsem.at[1], (me, near)).wait_recv()
    push(resq, resid.at[:, cols(near_far)], gssem.at[2], grsem.at[2], (me, near)).wait_recv()
    own.wait()
    for cp in waits:
        cp.wait_send()
    chain.finish()


def give_back(back, comb, og_q, normed, n_tp):
    n_sp, cap, width = back.shape
    q = width // n_tp
    tokens = og_q.shape[0]
    dma = pltpu.SemaphoreType.DMA
    block = pltpu.VMEM((n_sp, cap, q), BF16)
    return pl.pallas_call(
        functools.partial(return_kernel, n_sp, n_tp, q),
        out_shape=(
            jax.ShapeDtypeStruct((tokens, width), BF16),
            jax.ShapeDtypeStruct((n_sp,) + normed.shape, BF16),
        ),
        in_specs=vmem_specs(3) + any_specs(1),
        out_specs=tuple(any_specs(2)),
        scratch_shapes=[pltpu.VMEM((2, n_sp, cap, q), BF16)]
        + [block] * 4
        + [pltpu.VMEM((tokens, q), BF16)]
        + [dma((2, n_sp))] * 2
        + [dma((n_sp,))] * 4
        + [dma((4,)), dma((3,))]
        + chain_sems(n_sp),
        compiler_params=pltpu.CompilerParams(collective_id=1, has_side_effects=True),
        name="give_back",
    )(back, comb, og_q, normed)


def swap_kernel(n_sp, w, resid, state, cols_out, states, own_sem, ssem, rsem, *chain_sem):
    me = lax.axis_index("sp")
    c = lax.axis_index("tp")
    greet(n_sp, me, c, True, ())

    def part(index):
        if len(resid.shape) == 3:
            return resid.at[index]
        return resid.at[:, pl.ds(pl.multiple_of(index * w, 128), w)]

    chain = Chain(state, states, n_sp, me, c, chain_sem, (1,))
    chain.start()
    waits = []
    for k in range(1, n_sp):
        peer = lax.rem(me + k, n_sp)
        cp = push(part(peer), cols_out.at[me], ssem.at[k], rsem.at[k], (peer, c))
        cp.start()
        waits.append(cp)
    local = pltpu.make_async_copy(part(me), cols_out.at[me], own_sem.at[0])
    local.start()
    for d in range(1, n_sp // 2):
        chain.step(d)
    for k in range(1, n_sp):
        source = lax.rem(me + n_sp - k, n_sp)
        spot = cols_out.at[source]
        push(spot, spot, ssem.at[k], rsem.at[k], (source, c)).wait_recv()
    for cp in waits:
        cp.wait_send()
    local.wait()
    chain.finish()


def swap(resid, state, n_sp):
    tokens, width = resid.shape
    w = width // n_sp
    if w % 128:
        resid = resid.reshape(tokens, n_sp, w).transpose(1, 0, 2)
    dma = pltpu.SemaphoreType.DMA
    return pl.pallas_call(
        functools.partial(swap_kernel, n_sp, w),
        out_shape=(
            jax.ShapeDtypeStruct((n_sp, tokens, w), BF16),
            jax.ShapeDtypeStruct((n_sp,) + state.shape, BF16),
        ),
        in_specs=any_specs(2),
        out_specs=tuple(any_specs(2)),
        scratch_shapes=[dma((1,)), dma((n_sp,)), dma((n_sp,))] + chain_sems(n_sp),
        compiler_params=pltpu.CompilerParams(collective_id=2, has_side_effects=True),
        name="swap",
    )(resid, state)


def rotation_tables(start, count, key_width):
    frequency = 1.0 / 10000.0 ** jnp.linspace(0.0, 1.0, key_width // 2, dtype=F32)
    frequency = jnp.repeat(frequency, 2)
    token_position = (start + jnp.arange(count, dtype=jnp.int32)).astype(F32)
    angles = token_position[:, None] * frequency[None, :]
    return (jnp.cos(angles)[None], jnp.sin(angles)[None])


def swap_matrix(key_width):
    row = jnp.arange(key_width)[:, None]
    col = jnp.arange(key_width)[None, :]
    up = (col == row + 1) & (row % 2 == 0)
    down = (col == row - 1) & (row % 2 == 1)
    return (up.astype(F32) - down.astype(F32)).astype(BF16)


def turn(field, cosines, sines, matrix):
    turned = jnp.einsum("htk,kl->htl", field.astype(BF16), matrix, preferred_element_type=F32)
    return field.astype(F32) * cosines + turned * sines


def ein(spec, a, b):
    return jnp.einsum(spec, a.astype(BF16), b.astype(BF16), preferred_element_type=F32)


def fine(spec, a, b):
    return jnp.einsum(spec, a.astype(F32), b.astype(F32), precision=lax.Precision.HIGHEST)


def weighted(states, factors, present):
    kept = jnp.where(present[:, None, None, None], states.astype(F32), 0.0)
    return jnp.sum(kept * factors[:, :, None, None], axis=0)


def mm(a, b, da, db):
    return lax.dot_general(a, b, (((da,), (db,)), ((), ())), preferred_element_type=F32)


def expert_local(routed_rows, routed_grads, gate_w, up_w, down_w):
    gate_pre = mm(routed_rows, gate_w, 1, 0)
    up_pre = mm(routed_rows, up_w, 1, 0)
    gate_clip = jnp.minimum(gate_pre, CLAMP_LIMIT)
    up_clip = jnp.clip(up_pre, -CLAMP_LIMIT, CLAMP_LIMIT)
    sigmoid_gate = jax.nn.sigmoid(GATE_SLOPE * gate_clip)
    activated = (gate_clip * sigmoid_gate * (up_clip + 1.0)).astype(BF16)
    down_part = mm(activated, routed_grads, 0, 0)
    act_grad = mm(routed_grads, down_w, 1, 1)
    slope = sigmoid_gate + GATE_SLOPE * gate_clip * sigmoid_gate * (1.0 - sigmoid_gate)
    gate_pre_grad = jnp.where(
        gate_pre < CLAMP_LIMIT, act_grad * (up_clip + 1.0) * slope, 0.0
    ).astype(BF16)
    up_pre_grad = jnp.where(
        jnp.abs(up_pre) < CLAMP_LIMIT, act_grad * gate_clip * sigmoid_gate, 0.0
    ).astype(BF16)
    gate_part = mm(routed_rows, gate_pre_grad, 0, 0)
    up_part = mm(routed_rows, up_pre_grad, 0, 0)
    back_rows = mm(gate_pre_grad, gate_w, 1, 1) + mm(up_pre_grad, up_w, 1, 1)
    return (
        gate_part.astype(BF16),
        up_part.astype(BF16),
        down_part.astype(BF16),
        back_rows.astype(BF16),
    )


def per_device(
    stream, out_grad, routes, route_weight, queries, key_vectors, value_vectors, log_decay,
    out_proj, gate_weight, up_weight, down_weight,
):
    n_sp = lax.axis_size("sp")
    n_tp = lax.axis_size("tp")
    me = lax.axis_index("sp")
    tokens, width = stream.shape
    capacity = 4 * tokens // n_sp
    slots = n_sp * capacity
    quarter = width // n_tp
    heads = queries.shape[1]
    key_width = queries.shape[2]
    value_width = value_vectors.shape[2]

    ids = jnp.arange(n_sp, dtype=jnp.int32)
    chosen = routes[:, :, None] == ids[None, None, :]
    counts = jnp.sum(chosen.astype(F32), axis=1).astype(BF16)
    place = jnp.arange(tokens)
    lower = (place[:, None] > place[None, :]).astype(BF16)
    before = jnp.dot(lower, counts, preferred_element_type=F32)
    slot = jnp.sum(jnp.where(chosen, before[:, None, :], 0.0), axis=2).astype(jnp.int32)
    target = routes * capacity + slot
    spots = jnp.arange(slots, dtype=jnp.int32)
    hit = target.T[:, None, :] == spots[None, :, None]
    pick = (hit[0] | hit[1]).astype(BF16)
    weight = jnp.sum(
        jnp.where(hit[0], route_weight[None, :, 0], 0.0)
        + jnp.where(hit[1], route_weight[None, :, 1], 0.0),
        axis=1,
    )
    comb = ((target[:, :1] == spots[None, :]) | (target[:, 1:] == spots[None, :])).astype(BF16)
    col_start = lax.axis_index("tp") * quarter
    stream_q = lax.dynamic_slice_in_dim(stream, col_start, quarter, 1)
    og_q = lax.dynamic_slice_in_dim(out_grad, col_start, quarter, 1)
    send_rows = jnp.dot(pick, stream_q, preferred_element_type=F32).astype(BF16)
    send_grads = (
        weight[:, None] * jnp.dot(pick, og_q, preferred_element_type=F32)
    ).astype(BF16)

    running = jnp.cumsum(log_decay, axis=0).T
    block_total = running[:, -1]
    tot = jnp.broadcast_to(jnp.pad(block_total, (0, 128 - heads))[None, :], (8, 128))
    matrix = swap_matrix(key_width)
    cosines, sines = rotation_tables(me * tokens, tokens, key_width)
    scale = key_width ** (-0.5)
    query_rot = turn(queries.transpose(1, 0, 2), cosines, sines, matrix)
    key_rot = turn(key_vectors.transpose(1, 0, 2), cosines, sines, matrix) * scale
    values = value_vectors.transpose(1, 0, 2)
    causal = (place[:, None] >= place[None, :])[None]
    difference = running[:, :, None] - running[:, None, :]
    mask = jnp.where(causal, jnp.exp(jnp.where(causal, difference, 0.0)), 0.0)
    decay = jnp.exp(running)[..., None]
    remaining = jnp.exp(block_total[:, None] - running)[..., None]
    inner = ein("wfs,wfi->wsi", key_rot * remaining, values).astype(BF16)
    rows, grads, tots, inner_all = dispatch(
        send_rows.reshape(n_sp, capacity, quarter),
        send_grads.reshape(n_sp, capacity, quarter),
        tot,
        inner,
        n_tp,
    )
    key_bf = key_rot.astype(BF16)
    query_bf = query_rot.astype(BF16)
    weights = fine("hik,hjk->hij", query_rot, key_rot) * mask
    retained_local = fine("hij,hjv->hiv", weights, values)

    gate_part, up_part, down_part, back_rows = expert_local(
        rows.reshape(slots, width),
        grads.reshape(slots, width),
        gate_weight[0],
        up_weight[0],
        down_weight[0],
    )
    totals = tots[:, 0, :heads]
    sums = jnp.cumsum(totals, axis=0)
    sum_before = jnp.sum(jnp.where((ids < me)[:, None], totals, 0.0), axis=0)
    sum_through = sum_before + block_total
    past = jnp.where((ids < me)[:, None], sum_before[None] - sums, 0.0)
    past = jnp.where((ids < me)[:, None], jnp.exp(past), 0.0)
    coming = jnp.where((ids > me)[:, None], sums - totals - sum_through[None], 0.0)
    coming = jnp.where((ids > me)[:, None], jnp.exp(coming), 0.0)
    incoming = weighted(inner_all, past, ids < me)
    retained = retained_local + decay * fine("dzr,drs->dzs", query_rot, incoming)
    inverse_rms = lax.rsqrt(jnp.mean(retained * retained, axis=-1, keepdims=True) + EPSILON)
    normed = retained * inverse_rms
    normed_bf = normed.transpose(1, 0, 2).reshape(tokens, heads * value_width).astype(BF16)

    resid, normed_all = give_back(
        back_rows.reshape(n_sp, capacity, width), comb, og_q, normed_bf, n_tp
    )
    normed_grad = jnp.dot(resid, out_proj, preferred_element_type=F32)
    normed_grad = normed_grad.reshape(tokens, heads, value_width).transpose(1, 0, 2)
    grad = inverse_rms * (
        normed_grad - normed * jnp.mean(normed_grad * normed, axis=-1, keepdims=True)
    )
    grad_bf = grad.astype(BF16)
    inner_grad = ein("gwn,gwj->gnj", query_rot * decay, grad_bf).astype(BF16)
    resid_cols, grads_all = swap(resid, inner_grad, n_sp)
    future = weighted(grads_all, coming, ids > me).astype(BF16)
    score = fine("hiv,hjv->hij", grad, values) * mask
    query_portion = ein("hij,hjk->hik", score, key_bf) + decay * fine(
        "bpl,btl->bpt", grad, incoming
    )
    key_portion = ein("hij,hik->hjk", score, query_bf) + remaining * ein(
        "uxn,ubn->uxb", values, future
    )
    value_portion = ein("hij,hiv->hjv", weights, grad_bf) + remaining * ein(
        "bui,bim->bum", key_bf, future
    )
    query_grad = turn(query_portion, cosines, -sines, matrix).astype(BF16).transpose(1, 0, 2)
    key_grad = (
        (turn(key_portion, cosines, -sines, matrix) * scale).astype(BF16).transpose(1, 0, 2)
    )
    value_grad = value_portion.astype(BF16).transpose(1, 0, 2)
    proj_grad = mm(
        resid_cols.reshape(n_sp * tokens, -1), normed_all.reshape(n_sp * tokens, -1), 0, 0
    )
    return (
        gate_part[None],
        up_part[None],
        down_part[None],
        proj_grad,
        query_grad,
        key_grad,
        value_grad,
    )


def solution(mesh):
    in_specs = (
        P("sp", None),
        P("sp", None),
        P("sp", None),
        P("sp", None),
        P("sp", "tp", None),
        P("sp", "tp", None),
        P("sp", "tp", None),
        P("sp", "tp"),
        P(None, "tp"),
        P("sp", None, "tp"),
        P("sp", None, "tp"),
        P("sp", "tp", None),
    )
    out_specs = (
        P("sp", None, "tp"),
        P("sp", None, "tp"),
        P("sp", "tp", None),
        P("sp", "tp"),
        P("sp", "tp", None),
        P("sp", "tp", None),
        P("sp", "tp", None),
    )
    return jax.shard_map(
        per_device, mesh=mesh, in_specs=in_specs, out_specs=out_specs, check_vma=False
    )
```

```python
import functools

import jax
import jax.numpy as jnp
from jax import lax
from jax.experimental import pallas as pl
from jax.experimental.pallas import tpu as pltpu
from jax.sharding import PartitionSpec as P

CLAMP_LIMIT = 7.0
GATE_SLOPE = 1.702
EPSILON = 1e-06
F32 = jnp.float32
BF16 = jnp.bfloat16
MESH = pl.DeviceIdType.MESH


def any_specs(count):
    return [pl.BlockSpec(memory_space=pl.ANY)] * count


def vmem_specs(count):
    return [pl.BlockSpec(memory_space=pltpu.VMEM)] * count


def tp_partners(c, n_tp):
    far = lax.rem(c + n_tp // 2, n_tp)
    near = c + 1 - 2 * lax.rem(c, 2)
    return far, near


def greet(n_sp, me, c, sp_peers, tp_peers):
    barrier = pltpu.get_barrier_semaphore()
    count = 0
    if sp_peers:
        for k in range(1, n_sp):
            pl.semaphore_signal(
                barrier, inc=1, device_id=(lax.rem(me + k, n_sp), c), device_id_type=MESH
            )
            count += 1
    for t in tp_peers:
        pl.semaphore_signal(barrier, inc=1, device_id=(me, t), device_id_type=MESH)
        count += 1
    pl.semaphore_wait(barrier, count)


def push(src, dst, send_sem, recv_sem, device):
    return pltpu.make_async_remote_copy(
        src_ref=src,
        dst_ref=dst,
        send_sem=send_sem,
        recv_sem=recv_sem,
        device_id=device,
        device_id_type=MESH,
    )


class Chain:
    def __init__(self, src, out, n_sp, me, c, sems, ways):
        self.src, self.out, self.me, self.c = src, out, me, c
        self.pairs, self.ways = n_sp // 2, ways
        self.pair = me // 2
        self.other = me + 1 - 2 * lax.rem(me, 2)
        self.zs, self.zr, self.ys, self.yr, self.own_sem = sems

    def has(self, d, way):
        return self.pair >= d if way == 0 else self.pair + d < self.pairs

    def room(self, way):
        return self.pair + 1 < self.pairs if way == 0 else self.pair >= 1

    def spot(self, base, d, way):
        return self.out.at[base - 2 * d if way == 0 else base + 2 * d]

    def along(self, d, way):
        spot = self.spot(self.me, d, way)
        return push(
            self.src if d == 0 else spot, spot, self.zs.at[way, d], self.zr.at[way, d + 1],
            (self.me + 2 if way == 0 else self.me - 2, self.c),
        )

    def across(self, d, way):
        spot = self.spot(self.me, d, way)
        return push(
            self.src if d == 0 else spot, spot, self.ys.at[way, d], self.yr.at[way, d],
            (self.other, self.c),
        )

    def own(self):
        return pltpu.make_async_copy(self.src, self.out.at[self.me], self.own_sem.at[0])

    def each(self, d, act):
        for way in self.ways:

            @pl.when(self.has(d, way))
            def _():
                if d < self.pairs - 1:

                    @pl.when(self.room(way))
                    def _():
                        act(self.along(d, way))

                if d > 0 or way == self.ways[0]:
                    act(self.across(d, way))

    def start(self):
        self.own().start()
        self.each(0, lambda cp: cp.start())

    def step(self, d):
        for way in self.ways:

            @pl.when(self.has(d, way))
            def _():
                spot = self.spot(self.me, d, way)
                push(
                    spot, spot, self.zs.at[way, d], self.zr.at[way, d], (self.other, self.c)
                ).wait_recv()

        self.each(d, lambda cp: cp.start())

    def finish(self):
        for d in range(self.pairs):
            for way in self.ways:
                if d == 0 and way != self.ways[0]:
                    continue

                @pl.when(self.has(d, way))
                def _():
                    spot = self.spot(self.other, d, way)
                    push(
                        spot, spot, self.ys.at[way, d], self.yr.at[way, d], (self.other, self.c)
                    ).wait_recv()

            self.each(d, lambda cp: cp.wait_send())
        self.own().wait()


def chain_sems(n_sp):
    dma = pltpu.SemaphoreType.DMA
    return [dma((2, n_sp // 2))] * 4 + [dma((1,))]


def dispatch_kernel(
    n_sp, n_tp, q, rows, grads, tot, state, rows_out, grads_out, tot_out, states,
    own_sem, ssem, rsem, xssem, xrsem, dssem, drsem, essem, ersem, tssem, trsem, *chain_sem,
):
    me = lax.axis_index("sp")
    c = lax.axis_index("tp")
    far, near = tp_partners(c, n_tp)
    greet(n_sp, me, c, True, (far, near))
    arrays = ((rows, rows_out), (grads, grads_out))

    def cols(quarter):
        return pl.ds(pl.multiple_of(quarter * q, 128), q)

    chain = Chain(state, states, n_sp, me, c, chain_sem, (0,))
    chain.start()
    waits = []
    for k in range(1, n_sp):
        peer = lax.rem(me + k, n_sp)
        cp = push(tot, tot_out.at[me], tssem.at[k], trsem.at[k], (peer, c))
        cp.start()
        waits.append(cp)
        for a, (src, out) in enumerate(arrays):
            cp = push(
                src.at[peer], out.at[me, :, cols(c)], ssem.at[a, k], rsem.at[a, k], (peer, c)
            )
            cp.start()
            waits.append(cp)
    local = [pltpu.make_async_copy(tot, tot_out.at[me], own_sem.at[2])]
    for a, (src, out) in enumerate(arrays):
        local.append(pltpu.make_async_copy(src.at[me], out.at[me, :, cols(c)], own_sem.at[a]))
    for cp in local:
        cp.start()
    sent = []
    last = []

    def relay(k):
        source = lax.rem(me + n_sp - k, n_sp)
        for a, (src, out) in enumerate(arrays):
            spot = out.at[source, :, cols(far)]
            push(spot, spot, xssem.at[a, k], xrsem.at[a, k], (me, far)).wait_recv()
            cp = push(spot, spot, essem.at[a, k], ersem.at[a, k], (me, near))
            cp.start()
            sent.append(cp)
            last.append((out, source, a, k))

    for k in range(n_sp):
        source = lax.rem(me + n_sp - k, n_sp)
        for a, (src, out) in enumerate(arrays):
            spot = out.at[source, :, cols(c)]
            if k == 0:
                origin = src.at[me]
            else:
                push(spot, spot, ssem.at[a, k], rsem.at[a, k], (me, far)).wait_recv()
                origin = spot
            for sems, device in (((xssem, xrsem), far), ((dssem, drsem), near)):
                cp = push(origin, spot, sems[0].at[a, k], sems[1].at[a, k], (me, device))
                cp.start()
                sent.append(cp)
        if k >= 1:
            relay(k - 1)
        if k and k % 2 == 0:
            chain.step(k // 2)
    relay(n_sp - 1)
    near_far = lax.rem(near + n_tp // 2, n_tp)
    for out, source, a, k in last:
        spot = out.at[source, :, cols(near)]
        push(spot, spot, dssem.at[a, k], drsem.at[a, k], (me, near)).wait_recv()
        spot = out.at[source, :, cols(near_far)]
        push(spot, spot, essem.at[a, k], ersem.at[a, k], (me, near)).wait_recv()
    for k in range(1, n_sp):
        source = lax.rem(me + n_sp - k, n_sp)
        spot = tot_out.at[source]
        push(spot, spot, tssem.at[k], trsem.at[k], (me, far)).wait_recv()
    for cp in waits + sent:
        cp.wait_send()
    for cp in local:
        cp.wait()
    chain.finish()


def dispatch(rows, grads, tot, state, n_tp):
    n_sp, cap, q = rows.shape
    full = jax.ShapeDtypeStruct((n_sp, cap, q * n_tp), rows.dtype)
    dma = pltpu.SemaphoreType.DMA
    return pl.pallas_call(
        functools.partial(dispatch_kernel, n_sp, n_tp, q),
        out_shape=(
            full,
            full,
            jax.ShapeDtypeStruct((n_sp,) + tot.shape, tot.dtype),
            jax.ShapeDtypeStruct((n_sp,) + state.shape, state.dtype),
        ),
        in_specs=any_specs(4),
        out_specs=tuple(any_specs(4)),
        scratch_shapes=[dma((3,))] + [dma((2, n_sp))] * 8 + [dma((n_sp,))] * 2 + chain_sems(n_sp),
        compiler_params=pltpu.CompilerParams(collective_id=0, has_side_effects=True),
        name="dispatch",
    )(rows, grads, tot, state)


def return_kernel(
    n_sp, n_tp, q, back, comb, og, normed, resid, normed_all,
    part, xbuf, xrecv, sendbuf, ret, resq,
    pssem, prsem, xssem, xrsem, ssem, rsem, gssem, grsem, *chain_sem,
):
    me = lax.axis_index("sp")
    c = lax.axis_index("tp")
    far, near = tp_partners(c, n_tp)
    near_far = lax.rem(near + n_tp // 2, n_tp)
    greet(n_sp, me, c, True, (far, near))

    def cols(quarter):
        return pl.ds(pl.multiple_of(quarter * q, 128), q)

    order = list(range(1, n_sp)) + [0]
    waits = []
    for k in order:
        i = lax.rem(me + k, n_sp)
        for b, quarter in enumerate((near_far, near)):
            cp = push(
                back.at[i, :, cols(quarter)], part.at[b, k], pssem.at[b, k], prsem.at[b, k],
                (me, near),
            )
            cp.start()
            waits.append(cp)
    chain = Chain(normed, normed_all, n_sp, me, c, chain_sem, (0, 1))
    chain.start()

    def to_far(k):
        cp = push(xbuf.at[k], xrecv.at[k], xssem.at[k], xrsem.at[k], (me, far))
        cp.start()
        waits.append(cp)

    def to_home(k):
        cp = push(
            sendbuf.at[k], ret.at[me], ssem.at[k], rsem.at[k], (lax.rem(me + k, n_sp), c)
        )
        cp.start()
        waits.append(cp)

    def first(k):
        i = lax.rem(me + k, n_sp)
        push(xbuf.at[k], part.at[0, k], pssem.at[0, k], prsem.at[0, k], (me, near)).wait_recv()
        xbuf[k] = (back[i, :, cols(far)].astype(F32) + part[0, k].astype(F32)).astype(BF16)

    def second(k):
        i = lax.rem(me + k, n_sp)
        push(xbuf.at[k], part.at[1, k], pssem.at[1, k], prsem.at[1, k], (me, near)).wait_recv()
        push(xbuf.at[k], xrecv.at[k], xssem.at[k], xrsem.at[k], (me, far)).wait_recv()
        total = (
            back[i, :, cols(c)].astype(F32) + part[1, k].astype(F32) + xrecv[k].astype(F32)
        ).astype(BF16)
        if k == 0:
            ret[me] = total
        else:
            sendbuf[k] = total

    lag = 2
    for n in range(n_sp + lag + 1):
        if n < n_sp:
            first(order[n])
        if 1 <= n <= n_sp:
            to_far(order[n - 1])
        if lag <= n < n_sp + lag:
            second(order[n - lag])
        if n >= lag + 1 and order[n - lag - 1] != 0:
            to_home(order[n - lag - 1])
        if n and n % 3 == 0 and n // 3 < n_sp // 2:
            chain.step(n // 3)
    for d in range((n_sp + lag) // 3 + 1, n_sp // 2):
        chain.step(d)
    for k in range(1, n_sp):
        source = lax.rem(me + n_sp - k, n_sp)
        push(sendbuf.at[k], ret.at[source], ssem.at[k], rsem.at[k], (me, far)).wait_recv()
    cap = back.shape[1]
    returned = ret[...].astype(F32).reshape(n_sp * cap, q).astype(BF16)
    resq[...] = (
        og[...].astype(F32) + jnp.dot(comb[...], returned, preferred_element_type=F32)
    ).astype(BF16)
    mine = resid.at[:, cols(c)]
    own = pltpu.make_async_copy(resq, mine, gssem.at[3])
    own.start()
    for s, device in enumerate((far, near)):
        cp = push(resq, mine, gssem.at[s], grsem.at[s], (me, device))
        cp.start()
        waits.append(cp)
    spot = resid.at[:, cols(far)]
    push(resq, spot, gssem.at[0], grsem.at[0], (me, far)).wait_recv()
    cp = push(spot, spot, gssem.at[2], grsem.at[2], (me, near))
    cp.start()
    waits.append(cp)
    push(resq, resid.at[:, cols(near)], gssem.at[1], grsem.at[1], (me, near)).wait_recv()
    push(resq, resid.at[:, cols(near_far)], gssem.at[2], grsem.at[2], (me, near)).wait_recv()
    own.wait()
    for cp in waits:
        cp.wait_send()
    chain.finish()


def give_back(back, comb, og_q, normed, n_tp):
    n_sp, cap, width = back.shape
    q = width // n_tp
    tokens = og_q.shape[0]
    dma = pltpu.SemaphoreType.DMA
    block = pltpu.VMEM((n_sp, cap, q), BF16)
    return pl.pallas_call(
        functools.partial(return_kernel, n_sp, n_tp, q),
        out_shape=(
            jax.ShapeDtypeStruct((tokens, width), BF16),
            jax.ShapeDtypeStruct((n_sp,) + normed.shape, BF16),
        ),
        in_specs=vmem_specs(3) + any_specs(1),
        out_specs=tuple(any_specs(2)),
        scratch_shapes=[pltpu.VMEM((2, n_sp, cap, q), BF16)]
        + [block] * 4
        + [pltpu.VMEM((tokens, q), BF16)]
        + [dma((2, n_sp))] * 2
        + [dma((n_sp,))] * 4
        + [dma((4,)), dma((3,))]
        + chain_sems(n_sp),
        compiler_params=pltpu.CompilerParams(collective_id=1, has_side_effects=True),
        name="give_back",
    )(back, comb, og_q, normed)


def swap_kernel(
    n_sp, w, tile, resid, state, rows, grads, act, gate_back, up_back,
    cols_out, states, gate_out, up_out, down_out, own_sem, ssem, rsem, *chain_sem,
):
    me = lax.axis_index("sp")
    c = lax.axis_index("tp")
    greet(n_sp, me, c, True, ())

    def part(index):
        if len(resid.shape) == 3:
            return resid.at[index]
        return resid.at[:, pl.ds(pl.multiple_of(index * w, 128), w)]

    chain = Chain(state, states, n_sp, me, c, chain_sem, (1,))
    chain.start()
    waits = []

    def send(k):
        cp = push(
            part(lax.rem(me + k, n_sp)), cols_out.at[me], ssem.at[k], rsem.at[k],
            (lax.rem(me + k, n_sp), c),
        )
        cp.start()
        waits.append(cp)

    local = pltpu.make_async_copy(part(me), cols_out.at[me], own_sem.at[0])
    local.start()
    tiles = rows.shape[1] // tile

    def outer(lo, hi):
        @pl.loop(lo, hi)
        def _(i):
            span = pl.ds(pl.multiple_of(i * tile, tile), tile)
            gate_out[span, :] = mm(rows[:, span], gate_back[...], 0, 0).astype(BF16)
            up_out[span, :] = mm(rows[:, span], up_back[...], 0, 0).astype(BF16)
            down_out[:, span] = mm(act[...], grads[:, span], 0, 0).astype(BF16)

    steps = n_sp // 2
    for d in range(1, steps):
        send(2 * d)
        send(2 * d - 1)
        outer(tiles * (d - 1) // (steps - 1), tiles * d // (steps - 1))
        chain.step(d)
    send(n_sp - 1)
    for k in range(1, n_sp):
        source = lax.rem(me + n_sp - k, n_sp)
        spot = cols_out.at[source]
        push(spot, spot, ssem.at[k], rsem.at[k], (source, c)).wait_recv()
    for cp in waits:
        cp.wait_send()
    local.wait()
    chain.finish()


def swap(resid, state, rows, grads, act, gate_back, up_back, n_sp):
    tokens, width = resid.shape
    w = width // n_sp
    if w % 128:
        resid = resid.reshape(tokens, n_sp, w).transpose(1, 0, 2)
    hidden = act.shape[1]
    tile = width // 8
    dma = pltpu.SemaphoreType.DMA
    return pl.pallas_call(
        functools.partial(swap_kernel, n_sp, w, tile),
        out_shape=(
            jax.ShapeDtypeStruct((n_sp, tokens, w), BF16),
            jax.ShapeDtypeStruct((n_sp,) + state.shape, BF16),
            jax.ShapeDtypeStruct((width, hidden), BF16),
            jax.ShapeDtypeStruct((width, hidden), BF16),
            jax.ShapeDtypeStruct((hidden, width), BF16),
        ),
        in_specs=any_specs(2) + vmem_specs(5),
        out_specs=tuple(any_specs(2) + vmem_specs(3)),
        scratch_shapes=[dma((1,)), dma((n_sp,)), dma((n_sp,))] + chain_sems(n_sp),
        compiler_params=pltpu.CompilerParams(collective_id=2, has_side_effects=True),
        name="swap",
    )(resid, state, rows, grads, act, gate_back, up_back)


def rotation_tables(start, count, key_width):
    frequency = 1.0 / 10000.0 ** jnp.linspace(0.0, 1.0, key_width // 2, dtype=F32)
    frequency = jnp.repeat(frequency, 2)
    token_position = (start + jnp.arange(count, dtype=jnp.int32)).astype(F32)
    angles = token_position[:, None] * frequency[None, :]
    return (jnp.cos(angles)[None], jnp.sin(angles)[None])


def swap_matrix(key_width):
    row = jnp.arange(key_width)[:, None]
    col = jnp.arange(key_width)[None, :]
    up = (col == row + 1) & (row % 2 == 0)
    down = (col == row - 1) & (row % 2 == 1)
    return (up.astype(F32) - down.astype(F32)).astype(BF16)


def turn(field, cosines, sines, matrix):
    turned = jnp.einsum("htk,kl->htl", field.astype(BF16), matrix, preferred_element_type=F32)
    return field.astype(F32) * cosines + turned * sines


def ein(spec, a, b):
    return jnp.einsum(spec, a.astype(BF16), b.astype(BF16), preferred_element_type=F32)


def fine(spec, a, b):
    return jnp.einsum(spec, a.astype(F32), b.astype(F32), precision=lax.Precision.HIGHEST)


def weighted(states, factors, present):
    kept = jnp.where(present[:, None, None, None], states.astype(F32), 0.0)
    return jnp.sum(kept * factors[:, :, None, None], axis=0)


def mm(a, b, da, db):
    return lax.dot_general(a, b, (((da,), (db,)), ((), ())), preferred_element_type=F32)


def expert_local(routed_rows, routed_grads, gate_w, up_w, down_w):
    gate_pre = mm(routed_rows, gate_w, 1, 0)
    up_pre = mm(routed_rows, up_w, 1, 0)
    gate_clip = jnp.minimum(gate_pre, CLAMP_LIMIT)
    up_clip = jnp.clip(up_pre, -CLAMP_LIMIT, CLAMP_LIMIT)
    sigmoid_gate = jax.nn.sigmoid(GATE_SLOPE * gate_clip)
    activated = (gate_clip * sigmoid_gate * (up_clip + 1.0)).astype(BF16)
    act_grad = mm(routed_grads, down_w, 1, 1)
    slope = sigmoid_gate + GATE_SLOPE * gate_clip * sigmoid_gate * (1.0 - sigmoid_gate)
    gate_pre_grad = jnp.where(
        gate_pre < CLAMP_LIMIT, act_grad * (up_clip + 1.0) * slope, 0.0
    ).astype(BF16)
    up_pre_grad = jnp.where(
        jnp.abs(up_pre) < CLAMP_LIMIT, act_grad * gate_clip * sigmoid_gate, 0.0
    ).astype(BF16)
    back_rows = mm(gate_pre_grad, gate_w, 1, 1) + mm(up_pre_grad, up_w, 1, 1)
    return activated, gate_pre_grad, up_pre_grad, back_rows.astype(BF16)


def per_device(
    stream, out_grad, routes, route_weight, queries, key_vectors, value_vectors, log_decay,
    out_proj, gate_weight, up_weight, down_weight,
):
    n_sp = lax.axis_size("sp")
    n_tp = lax.axis_size("tp")
    me = lax.axis_index("sp")
    tokens, width = stream.shape
    capacity = 4 * tokens // n_sp
    slots = n_sp * capacity
    quarter = width // n_tp
    heads = queries.shape[1]
    key_width = queries.shape[2]
    value_width = value_vectors.shape[2]

    ids = jnp.arange(n_sp, dtype=jnp.int32)
    chosen = routes[:, :, None] == ids[None, None, :]
    counts = jnp.sum(chosen.astype(F32), axis=1).astype(BF16)
    place = jnp.arange(tokens)
    lower = (place[:, None] > place[None, :]).astype(BF16)
    before = jnp.dot(lower, counts, preferred_element_type=F32)
    slot = jnp.sum(jnp.where(chosen, before[:, None, :], 0.0), axis=2).astype(jnp.int32)
    target = routes * capacity + slot
    spots = jnp.arange(slots, dtype=jnp.int32)
    hit = target.T[:, None, :] == spots[None, :, None]
    pick = (hit[0] | hit[1]).astype(BF16)
    weight = jnp.sum(
        jnp.where(hit[0], route_weight[None, :, 0], 0.0)
        + jnp.where(hit[1], route_weight[None, :, 1], 0.0),
        axis=1,
    )
    comb = ((target[:, :1] == spots[None, :]) | (target[:, 1:] == spots[None, :])).astype(BF16)
    col_start = lax.axis_index("tp") * quarter
    stream_q = lax.dynamic_slice_in_dim(stream, col_start, quarter, 1)
    og_q = lax.dynamic_slice_in_dim(out_grad, col_start, quarter, 1)
    send_rows = jnp.dot(pick, stream_q, preferred_element_type=F32).astype(BF16)
    send_grads = (
        weight[:, None] * jnp.dot(pick, og_q, preferred_element_type=F32)
    ).astype(BF16)

    running = jnp.cumsum(log_decay, axis=0).T
    block_total = running[:, -1]
    tot = jnp.broadcast_to(jnp.pad(block_total, (0, 128 - heads))[None, :], (8, 128))
    matrix = swap_matrix(key_width)
    cosines, sines = rotation_tables(me * tokens, tokens, key_width)
    scale = key_width ** (-0.5)
    query_rot = turn(queries.transpose(1, 0, 2), cosines, sines, matrix)
    key_rot = turn(key_vectors.transpose(1, 0, 2), cosines, sines, matrix) * scale
    values = value_vectors.transpose(1, 0, 2)
    causal = (place[:, None] >= place[None, :])[None]
    difference = running[:, :, None] - running[:, None, :]
    mask = jnp.where(causal, jnp.exp(jnp.where(causal, difference, 0.0)), 0.0)
    decay = jnp.exp(running)[..., None]
    remaining = jnp.exp(block_total[:, None] - running)[..., None]
    inner = ein("wfs,wfi->wsi", key_rot * remaining, values).astype(BF16)
    rows, grads, tots, inner_all = dispatch(
        send_rows.reshape(n_sp, capacity, quarter),
        send_grads.reshape(n_sp, capacity, quarter),
        tot,
        inner,
        n_tp,
    )
    key_bf = key_rot.astype(BF16)
    query_bf = query_rot.astype(BF16)
    weights = fine("hik,hjk->hij", query_rot, key_rot) * mask
    retained_local = fine("hij,hjv->hiv", weights, values)

    activated, gate_back, up_back, back_rows = expert_local(
        rows.reshape(slots, width),
        grads.reshape(slots, width),
        gate_weight[0],
        up_weight[0],
        down_weight[0],
    )
    totals = tots[:, 0, :heads]
    sums = jnp.cumsum(totals, axis=0)
    sum_before = jnp.sum(jnp.where((ids < me)[:, None], totals, 0.0), axis=0)
    sum_through = sum_before + block_total
    past = jnp.where((ids < me)[:, None], sum_before[None] - sums, 0.0)
    past = jnp.where((ids < me)[:, None], jnp.exp(past), 0.0)
    coming = jnp.where((ids > me)[:, None], sums - totals - sum_through[None], 0.0)
    coming = jnp.where((ids > me)[:, None], jnp.exp(coming), 0.0)
    incoming = weighted(inner_all, past, ids < me)
    retained = retained_local + decay * fine("dzr,drs->dzs", query_rot, incoming)
    inverse_rms = lax.rsqrt(jnp.mean(retained * retained, axis=-1, keepdims=True) + EPSILON)
    normed = retained * inverse_rms
    normed_bf = normed.transpose(1, 0, 2).reshape(tokens, heads * value_width).astype(BF16)

    resid, normed_all = give_back(
        back_rows.reshape(n_sp, capacity, width), comb, og_q, normed_bf, n_tp
    )
    normed_grad = jnp.dot(resid, out_proj, preferred_element_type=F32)
    normed_grad = normed_grad.reshape(tokens, heads, value_width).transpose(1, 0, 2)
    grad = inverse_rms * (
        normed_grad - normed * jnp.mean(normed_grad * normed, axis=-1, keepdims=True)
    )
    grad_bf = grad.astype(BF16)
    inner_grad = ein("gwn,gwj->gnj", query_rot * decay, grad_bf).astype(BF16)
    resid_cols, grads_all, gate_part, up_part, down_part = swap(
        resid,
        inner_grad,
        rows.reshape(slots, width),
        grads.reshape(slots, width),
        activated,
        gate_back,
        up_back,
        n_sp,
    )
    future = weighted(grads_all, coming, ids > me).astype(BF16)
    score = fine("hiv,hjv->hij", grad, values) * mask
    query_portion = ein("hij,hjk->hik", score, key_bf) + decay * fine(
        "bpl,btl->bpt", grad, incoming
    )
    key_portion = ein("hij,hik->hjk", score, query_bf) + remaining * ein(
        "uxn,ubn->uxb", values, future
    )
    value_portion = ein("hij,hiv->hjv", weights, grad_bf) + remaining * ein(
        "bui,bim->bum", key_bf, future
    )
    query_grad = turn(query_portion, cosines, -sines, matrix).astype(BF16).transpose(1, 0, 2)
    key_grad = (
        (turn(key_portion, cosines, -sines, matrix) * scale).astype(BF16).transpose(1, 0, 2)
    )
    value_grad = value_portion.astype(BF16).transpose(1, 0, 2)
    proj_grad = mm(
        resid_cols.reshape(n_sp * tokens, -1), normed_all.reshape(n_sp * tokens, -1), 0, 0
    )
    return (
        gate_part[None],
        up_part[None],
        down_part[None],
        proj_grad,
        query_grad,
        key_grad,
        value_grad,
    )


def solution(mesh):
    in_specs = (
        P("sp", None),
        P("sp", None),
        P("sp", None),
        P("sp", None),
        P("sp", "tp", None),
        P("sp", "tp", None),
        P("sp", "tp", None),
        P("sp", "tp"),
        P(None, "tp"),
        P("sp", None, "tp"),
        P("sp", None, "tp"),
        P("sp", "tp", None),
    )
    out_specs = (
        P("sp", None, "tp"),
        P("sp", None, "tp"),
        P("sp", "tp", None),
        P("sp", "tp"),
        P("sp", "tp", None),
        P("sp", "tp", None),
        P("sp", "tp", None),
    )
    return jax.shard_map(
        per_device, mesh=mesh, in_specs=in_specs, out_specs=out_specs, check_vma=False
    )
```

```python
import functools

import jax
import jax.numpy as jnp
from jax import lax
from jax.experimental import pallas as pl
from jax.experimental.pallas import tpu as pltpu
from jax.sharding import PartitionSpec as P

CLAMP_LIMIT = 7.0
GATE_SLOPE = 1.702
EPSILON = 1e-06
F32 = jnp.float32
BF16 = jnp.bfloat16
MESH = pl.DeviceIdType.MESH


def any_specs(count):
    return [pl.BlockSpec(memory_space=pl.ANY)] * count


def vmem_specs(count):
    return [pl.BlockSpec(memory_space=pltpu.VMEM)] * count


def tp_partners(c, n_tp):
    far = lax.rem(c + n_tp // 2, n_tp)
    near = c + 1 - 2 * lax.rem(c, 2)
    return far, near


def greet(n_sp, me, c, sp_peers, tp_peers):
    barrier = pltpu.get_barrier_semaphore()
    count = 0
    if sp_peers:
        for k in range(1, n_sp):
            pl.semaphore_signal(
                barrier, inc=1, device_id=(lax.rem(me + k, n_sp), c), device_id_type=MESH
            )
            count += 1
    for t in tp_peers:
        pl.semaphore_signal(barrier, inc=1, device_id=(me, t), device_id_type=MESH)
        count += 1
    pl.semaphore_wait(barrier, count)


def push(src, dst, send_sem, recv_sem, device):
    return pltpu.make_async_remote_copy(
        src_ref=src,
        dst_ref=dst,
        send_sem=send_sem,
        recv_sem=recv_sem,
        device_id=device,
        device_id_type=MESH,
    )


class Chain:
    def __init__(self, src, out, n_sp, me, c, sems, ways):
        self.src, self.out, self.me, self.c = src, out, me, c
        self.pairs, self.ways = n_sp // 2, ways
        self.pair = me // 2
        self.other = me + 1 - 2 * lax.rem(me, 2)
        self.zs, self.zr, self.ys, self.yr, self.own_sem = sems

    def has(self, d, way):
        return self.pair >= d if way == 0 else self.pair + d < self.pairs

    def room(self, way):
        return self.pair + 1 < self.pairs if way == 0 else self.pair >= 1

    def spot(self, base, d, way):
        return self.out.at[base - 2 * d if way == 0 else base + 2 * d]

    def along(self, d, way):
        spot = self.spot(self.me, d, way)
        return push(
            self.src if d == 0 else spot, spot, self.zs.at[way, d], self.zr.at[way, d + 1],
            (self.me + 2 if way == 0 else self.me - 2, self.c),
        )

    def across(self, d, way):
        spot = self.spot(self.me, d, way)
        return push(
            self.src if d == 0 else spot, spot, self.ys.at[way, d], self.yr.at[way, d],
            (self.other, self.c),
        )

    def own(self):
        return pltpu.make_async_copy(self.src, self.out.at[self.me], self.own_sem.at[0])

    def each(self, d, act):
        for way in self.ways:

            @pl.when(self.has(d, way))
            def _():
                if d < self.pairs - 1:

                    @pl.when(self.room(way))
                    def _():
                        act(self.along(d, way))

                if d > 0 or way == self.ways[0]:
                    act(self.across(d, way))

    def start(self):
        self.own().start()
        self.each(0, lambda cp: cp.start())

    def step(self, d):
        for way in self.ways:

            @pl.when(self.has(d, way))
            def _():
                spot = self.spot(self.me, d, way)
                push(
                    spot, spot, self.zs.at[way, d], self.zr.at[way, d], (self.other, self.c)
                ).wait_recv()

        self.each(d, lambda cp: cp.start())

    def finish(self):
        for d in range(self.pairs):
            for way in self.ways:
                if d == 0 and way != self.ways[0]:
                    continue

                @pl.when(self.has(d, way))
                def _():
                    spot = self.spot(self.other, d, way)
                    push(
                        spot, spot, self.ys.at[way, d], self.yr.at[way, d], (self.other, self.c)
                    ).wait_recv()

            self.each(d, lambda cp: cp.wait_send())
        self.own().wait()


def chain_sems(n_sp):
    dma = pltpu.SemaphoreType.DMA
    return [dma((2, n_sp // 2))] * 4 + [dma((1,))]


def dispatch_kernel(
    n_sp, n_tp, q, rows, grads, tot, state, rows_out, grads_out, tot_out, states,
    own_sem, ssem, rsem, xssem, xrsem, dssem, drsem, essem, ersem, tssem, trsem, *chain_sem,
):
    me = lax.axis_index("sp")
    c = lax.axis_index("tp")
    far, near = tp_partners(c, n_tp)
    greet(n_sp, me, c, True, (far, near))
    arrays = ((rows, rows_out), (grads, grads_out))

    def cols(quarter):
        return pl.ds(pl.multiple_of(quarter * q, 128), q)

    chain = Chain(state, states, n_sp, me, c, chain_sem, (0,))
    chain.start()
    waits = []
    for k in range(1, n_sp):
        peer = lax.rem(me + k, n_sp)
        cp = push(tot, tot_out.at[me], tssem.at[k], trsem.at[k], (peer, c))
        cp.start()
        waits.append(cp)
        for a, (src, out) in enumerate(arrays):
            cp = push(
                src.at[peer], out.at[me, :, cols(c)], ssem.at[a, k], rsem.at[a, k], (peer, c)
            )
            cp.start()
            waits.append(cp)
    local = [pltpu.make_async_copy(tot, tot_out.at[me], own_sem.at[2])]
    for a, (src, out) in enumerate(arrays):
        local.append(pltpu.make_async_copy(src.at[me], out.at[me, :, cols(c)], own_sem.at[a]))
    for cp in local:
        cp.start()
    sent = []
    last = []

    def relay(k):
        source = lax.rem(me + n_sp - k, n_sp)
        for a, (src, out) in enumerate(arrays):
            spot = out.at[source, :, cols(far)]
            push(spot, spot, xssem.at[a, k], xrsem.at[a, k], (me, far)).wait_recv()
            cp = push(spot, spot, essem.at[a, k], ersem.at[a, k], (me, near))
            cp.start()
            sent.append(cp)
            last.append((out, source, a, k))

    for k in range(n_sp):
        source = lax.rem(me + n_sp - k, n_sp)
        for a, (src, out) in enumerate(arrays):
            spot = out.at[source, :, cols(c)]
            if k == 0:
                origin = src.at[me]
            else:
                push(spot, spot, ssem.at[a, k], rsem.at[a, k], (me, far)).wait_recv()
                origin = spot
            for sems, device in (((xssem, xrsem), far), ((dssem, drsem), near)):
                cp = push(origin, spot, sems[0].at[a, k], sems[1].at[a, k], (me, device))
                cp.start()
                sent.append(cp)
        if k >= 1:
            relay(k - 1)
        if k and k % 2 == 0:
            chain.step(k // 2)
    relay(n_sp - 1)
    near_far = lax.rem(near + n_tp // 2, n_tp)
    for out, source, a, k in last:
        spot = out.at[source, :, cols(near)]
        push(spot, spot, dssem.at[a, k], drsem.at[a, k], (me, near)).wait_recv()
        spot = out.at[source, :, cols(near_far)]
        push(spot, spot, essem.at[a, k], ersem.at[a, k], (me, near)).wait_recv()
    for k in range(1, n_sp):
        source = lax.rem(me + n_sp - k, n_sp)
        spot = tot_out.at[source]
        push(spot, spot, tssem.at[k], trsem.at[k], (me, far)).wait_recv()
    for cp in waits + sent:
        cp.wait_send()
    for cp in local:
        cp.wait()
    chain.finish()


def dispatch(rows, grads, tot, state, n_tp):
    n_sp, cap, q = rows.shape
    full = jax.ShapeDtypeStruct((n_sp, cap, q * n_tp), rows.dtype)
    dma = pltpu.SemaphoreType.DMA
    return pl.pallas_call(
        functools.partial(dispatch_kernel, n_sp, n_tp, q),
        out_shape=(
            full,
            full,
            jax.ShapeDtypeStruct((n_sp,) + tot.shape, tot.dtype),
            jax.ShapeDtypeStruct((n_sp,) + state.shape, state.dtype),
        ),
        in_specs=any_specs(4),
        out_specs=tuple(any_specs(4)),
        scratch_shapes=[dma((3,))] + [dma((2, n_sp))] * 8 + [dma((n_sp,))] * 2 + chain_sems(n_sp),
        compiler_params=pltpu.CompilerParams(collective_id=0, has_side_effects=True),
        name="dispatch",
    )(rows, grads, tot, state)


def return_kernel(
    n_sp, n_tp, q, back, comb, og, normed, resid, normed_all,
    part, xbuf, xrecv, sendbuf, ret, resq,
    pssem, prsem, xssem, xrsem, ssem, rsem, gssem, grsem, *chain_sem,
):
    me = lax.axis_index("sp")
    c = lax.axis_index("tp")
    far, near = tp_partners(c, n_tp)
    near_far = lax.rem(near + n_tp // 2, n_tp)
    greet(n_sp, me, c, True, (far, near))

    def cols(quarter):
        return pl.ds(pl.multiple_of(quarter * q, 128), q)

    order = list(range(1, n_sp)) + [0]
    waits = []
    for k in order:
        i = lax.rem(me + k, n_sp)
        for b, quarter in enumerate((near_far, near)):
            cp = push(
                back.at[i, :, cols(quarter)], part.at[b, k], pssem.at[b, k], prsem.at[b, k],
                (me, near),
            )
            cp.start()
            waits.append(cp)
    chain = Chain(normed, normed_all, n_sp, me, c, chain_sem, (0, 1))
    chain.start()

    def to_far(k):
        cp = push(xbuf.at[k], xrecv.at[k], xssem.at[k], xrsem.at[k], (me, far))
        cp.start()
        waits.append(cp)

    def to_home(k):
        cp = push(
            sendbuf.at[k], ret.at[me], ssem.at[k], rsem.at[k], (lax.rem(me + k, n_sp), c)
        )
        cp.start()
        waits.append(cp)

    def first(k):
        i = lax.rem(me + k, n_sp)
        push(xbuf.at[k], part.at[0, k], pssem.at[0, k], prsem.at[0, k], (me, near)).wait_recv()
        xbuf[k] = (back[i, :, cols(far)].astype(F32) + part[0, k].astype(F32)).astype(BF16)

    def second(k):
        i = lax.rem(me + k, n_sp)
        push(xbuf.at[k], part.at[1, k], pssem.at[1, k], prsem.at[1, k], (me, near)).wait_recv()
        push(xbuf.at[k], xrecv.at[k], xssem.at[k], xrsem.at[k], (me, far)).wait_recv()
        total = (
            back[i, :, cols(c)].astype(F32) + part[1, k].astype(F32) + xrecv[k].astype(F32)
        ).astype(BF16)
        if k == 0:
            ret[me] = total
        else:
            sendbuf[k] = total

    lag = 2
    for n in range(n_sp + lag + 1):
        if n < n_sp:
            first(order[n])
        if 1 <= n <= n_sp:
            to_far(order[n - 1])
        if lag <= n < n_sp + lag:
            second(order[n - lag])
        if n >= lag + 1 and order[n - lag - 1] != 0:
            to_home(order[n - lag - 1])
        if n and n % 3 == 0 and n // 3 < n_sp // 2:
            chain.step(n // 3)
    for d in range((n_sp + lag) // 3 + 1, n_sp // 2):
        chain.step(d)
    for k in range(1, n_sp):
        source = lax.rem(me + n_sp - k, n_sp)
        push(sendbuf.at[k], ret.at[source], ssem.at[k], rsem.at[k], (me, far)).wait_recv()
    cap = back.shape[1]
    returned = ret[...].astype(F32).reshape(n_sp * cap, q).astype(BF16)
    resq[...] = (
        og[...].astype(F32) + jnp.dot(comb[...], returned, preferred_element_type=F32)
    ).astype(BF16)
    mine = resid.at[:, cols(c)]
    own = pltpu.make_async_copy(resq, mine, gssem.at[3])
    own.start()
    for s, device in enumerate((far, near)):
        cp = push(resq, mine, gssem.at[s], grsem.at[s], (me, device))
        cp.start()
        waits.append(cp)
    spot = resid.at[:, cols(far)]
    push(resq, spot, gssem.at[0], grsem.at[0], (me, far)).wait_recv()
    cp = push(spot, spot, gssem.at[2], grsem.at[2], (me, near))
    cp.start()
    waits.append(cp)
    push(resq, resid.at[:, cols(near)], gssem.at[1], grsem.at[1], (me, near)).wait_recv()
    push(resq, resid.at[:, cols(near_far)], gssem.at[2], grsem.at[2], (me, near)).wait_recv()
    own.wait()
    for cp in waits:
        cp.wait_send()
    chain.finish()


def give_back(back, comb, og_q, normed, n_tp):
    n_sp, cap, width = back.shape
    q = width // n_tp
    tokens = og_q.shape[0]
    dma = pltpu.SemaphoreType.DMA
    block = pltpu.VMEM((n_sp, cap, q), BF16)
    return pl.pallas_call(
        functools.partial(return_kernel, n_sp, n_tp, q),
        out_shape=(
            jax.ShapeDtypeStruct((tokens, width), BF16),
            jax.ShapeDtypeStruct((n_sp,) + normed.shape, BF16),
        ),
        in_specs=vmem_specs(3) + any_specs(1),
        out_specs=tuple(any_specs(2)),
        scratch_shapes=[pltpu.VMEM((2, n_sp, cap, q), BF16)]
        + [block] * 4
        + [pltpu.VMEM((tokens, q), BF16)]
        + [dma((2, n_sp))] * 2
        + [dma((n_sp,))] * 4
        + [dma((4,)), dma((3,))]
        + chain_sems(n_sp),
        compiler_params=pltpu.CompilerParams(collective_id=1, has_side_effects=True),
        name="give_back",
    )(back, comb, og_q, normed)


def swap_kernel(n_sp, w, resid, state, cols_out, states, own_sem, ssem, rsem, *chain_sem):
    me = lax.axis_index("sp")
    c = lax.axis_index("tp")
    greet(n_sp, me, c, True, ())

    def part(index):
        if len(resid.shape) == 3:
            return resid.at[index]
        return resid.at[:, pl.ds(pl.multiple_of(index * w, 128), w)]

    chain = Chain(state, states, n_sp, me, c, chain_sem, (1,))
    chain.start()
    waits = []

    def send(k):
        peer = lax.rem(me + k, n_sp)
        cp = push(part(peer), cols_out.at[me], ssem.at[k], rsem.at[k], (peer, c))
        cp.start()
        waits.append(cp)

    local = pltpu.make_async_copy(part(me), cols_out.at[me], own_sem.at[0])
    local.start()
    for d in range(1, n_sp // 2):
        send(2 * d)
        send(2 * d - 1)
        chain.step(d)
    send(n_sp - 1)
    for k in range(1, n_sp):
        source = lax.rem(me + n_sp - k, n_sp)
        spot = cols_out.at[source]
        push(spot, spot, ssem.at[k], rsem.at[k], (source, c)).wait_recv()
    for cp in waits:
        cp.wait_send()
    local.wait()
    chain.finish()


def swap(resid, state, n_sp):
    tokens, width = resid.shape
    w = width // n_sp
    if w % 128:
        resid = resid.reshape(tokens, n_sp, w).transpose(1, 0, 2)
    dma = pltpu.SemaphoreType.DMA
    return pl.pallas_call(
        functools.partial(swap_kernel, n_sp, w),
        out_shape=(
            jax.ShapeDtypeStruct((n_sp, tokens, w), BF16),
            jax.ShapeDtypeStruct((n_sp,) + state.shape, BF16),
        ),
        in_specs=any_specs(2),
        out_specs=tuple(any_specs(2)),
        scratch_shapes=[dma((1,)), dma((n_sp,)), dma((n_sp,))] + chain_sems(n_sp),
        compiler_params=pltpu.CompilerParams(collective_id=2, has_side_effects=True),
        name="swap",
    )(resid, state)


def rotation_tables(start, count, key_width):
    frequency = 1.0 / 10000.0 ** jnp.linspace(0.0, 1.0, key_width // 2, dtype=F32)
    frequency = jnp.repeat(frequency, 2)
    token_position = (start + jnp.arange(count, dtype=jnp.int32)).astype(F32)
    angles = token_position[:, None] * frequency[None, :]
    return (jnp.cos(angles)[None], jnp.sin(angles)[None])


def swap_matrix(key_width):
    row = jnp.arange(key_width)[:, None]
    col = jnp.arange(key_width)[None, :]
    up = (col == row + 1) & (row % 2 == 0)
    down = (col == row - 1) & (row % 2 == 1)
    return (up.astype(F32) - down.astype(F32)).astype(BF16)


def turn(field, cosines, sines, matrix):
    turned = jnp.einsum("htk,kl->htl", field.astype(BF16), matrix, preferred_element_type=F32)
    return field.astype(F32) * cosines + turned * sines


def ein(spec, a, b):
    return jnp.einsum(spec, a.astype(BF16), b.astype(BF16), preferred_element_type=F32)


def fine(spec, a, b):
    return jnp.einsum(spec, a.astype(F32), b.astype(F32), precision=lax.Precision.HIGHEST)


def weighted(states, factors, present):
    kept = jnp.where(present[:, None, None, None], states.astype(F32), 0.0)
    return jnp.sum(kept * factors[:, :, None, None], axis=0)


def mm(a, b, da, db):
    return lax.dot_general(a, b, (((da,), (db,)), ((), ())), preferred_element_type=F32)


def expert_local(routed_rows, routed_grads, gate_w, up_w, down_w):
    gate_pre = mm(routed_rows, gate_w, 1, 0)
    up_pre = mm(routed_rows, up_w, 1, 0)
    gate_clip = jnp.minimum(gate_pre, CLAMP_LIMIT)
    up_clip = jnp.clip(up_pre, -CLAMP_LIMIT, CLAMP_LIMIT)
    sigmoid_gate = jax.nn.sigmoid(GATE_SLOPE * gate_clip)
    activated = (gate_clip * sigmoid_gate * (up_clip + 1.0)).astype(BF16)
    down_part = mm(activated, routed_grads, 0, 0)
    act_grad = mm(routed_grads, down_w, 1, 1)
    slope = sigmoid_gate + GATE_SLOPE * gate_clip * sigmoid_gate * (1.0 - sigmoid_gate)
    gate_pre_grad = jnp.where(
        gate_pre < CLAMP_LIMIT, act_grad * (up_clip + 1.0) * slope, 0.0
    ).astype(BF16)
    up_pre_grad = jnp.where(
        jnp.abs(up_pre) < CLAMP_LIMIT, act_grad * gate_clip * sigmoid_gate, 0.0
    ).astype(BF16)
    gate_part = mm(routed_rows, gate_pre_grad, 0, 0)
    up_part = mm(routed_rows, up_pre_grad, 0, 0)
    back_rows = mm(gate_pre_grad, gate_w, 1, 1) + mm(up_pre_grad, up_w, 1, 1)
    return (
        gate_part.astype(BF16),
        up_part.astype(BF16),
        down_part.astype(BF16),
        back_rows.astype(BF16),
    )


def per_device(
    stream, out_grad, routes, route_weight, queries, key_vectors, value_vectors, log_decay,
    out_proj, gate_weight, up_weight, down_weight,
):
    n_sp = lax.axis_size("sp")
    n_tp = lax.axis_size("tp")
    me = lax.axis_index("sp")
    tokens, width = stream.shape
    capacity = 4 * tokens // n_sp
    slots = n_sp * capacity
    quarter = width // n_tp
    heads = queries.shape[1]
    key_width = queries.shape[2]
    value_width = value_vectors.shape[2]

    ids = jnp.arange(n_sp, dtype=jnp.int32)
    chosen = routes[:, :, None] == ids[None, None, :]
    counts = jnp.sum(chosen.astype(F32), axis=1).astype(BF16)
    place = jnp.arange(tokens)
    lower = (place[:, None] > place[None, :]).astype(BF16)
    before = jnp.dot(lower, counts, preferred_element_type=F32)
    slot = jnp.sum(jnp.where(chosen, before[:, None, :], 0.0), axis=2).astype(jnp.int32)
    target = routes * capacity + slot
    spots = jnp.arange(slots, dtype=jnp.int32)
    hit = target.T[:, None, :] == spots[None, :, None]
    pick = (hit[0] | hit[1]).astype(BF16)
    weight = jnp.sum(
        jnp.where(hit[0], route_weight[None, :, 0], 0.0)
        + jnp.where(hit[1], route_weight[None, :, 1], 0.0),
        axis=1,
    )
    comb = ((target[:, :1] == spots[None, :]) | (target[:, 1:] == spots[None, :])).astype(BF16)
    col_start = lax.axis_index("tp") * quarter
    stream_q = lax.dynamic_slice_in_dim(stream, col_start, quarter, 1)
    og_q = lax.dynamic_slice_in_dim(out_grad, col_start, quarter, 1)
    send_rows = jnp.dot(pick, stream_q, preferred_element_type=F32).astype(BF16)
    send_grads = (
        weight[:, None] * jnp.dot(pick, og_q, preferred_element_type=F32)
    ).astype(BF16)

    running = jnp.cumsum(log_decay, axis=0).T
    block_total = running[:, -1]
    tot = jnp.broadcast_to(jnp.pad(block_total, (0, 128 - heads))[None, :], (8, 128))
    matrix = swap_matrix(key_width)
    cosines, sines = rotation_tables(me * tokens, tokens, key_width)
    scale = key_width ** (-0.5)
    query_rot = turn(queries.transpose(1, 0, 2), cosines, sines, matrix)
    key_rot = turn(key_vectors.transpose(1, 0, 2), cosines, sines, matrix) * scale
    values = value_vectors.transpose(1, 0, 2)
    causal = (place[:, None] >= place[None, :])[None]
    difference = running[:, :, None] - running[:, None, :]
    mask = jnp.where(causal, jnp.exp(jnp.where(causal, difference, 0.0)), 0.0)
    decay = jnp.exp(running)[..., None]
    remaining = jnp.exp(block_total[:, None] - running)[..., None]
    inner = ein("wfs,wfi->wsi", key_rot * remaining, values).astype(BF16)
    rows, grads, tots, inner_all = dispatch(
        send_rows.reshape(n_sp, capacity, quarter),
        send_grads.reshape(n_sp, capacity, quarter),
        tot,
        inner,
        n_tp,
    )
    key_bf = key_rot.astype(BF16)
    query_bf = query_rot.astype(BF16)
    weights = fine("hik,hjk->hij", query_rot, key_rot) * mask
    retained_local = fine("hij,hjv->hiv", weights, values)

    gate_part, up_part, down_part, back_rows = expert_local(
        rows.reshape(slots, width),
        grads.reshape(slots, width),
        gate_weight[0],
        up_weight[0],
        down_weight[0],
    )
    totals = tots[:, 0, :heads]
    sums = jnp.cumsum(totals, axis=0)
    sum_before = jnp.sum(jnp.where((ids < me)[:, None], totals, 0.0), axis=0)
    sum_through = sum_before + block_total
    past = jnp.where((ids < me)[:, None], sum_before[None] - sums, 0.0)
    past = jnp.where((ids < me)[:, None], jnp.exp(past), 0.0)
    coming = jnp.where((ids > me)[:, None], sums - totals - sum_through[None], 0.0)
    coming = jnp.where((ids > me)[:, None], jnp.exp(coming), 0.0)
    incoming = weighted(inner_all, past, ids < me)
    retained = retained_local + decay * fine("dzr,drs->dzs", query_rot, incoming)
    inverse_rms = lax.rsqrt(jnp.mean(retained * retained, axis=-1, keepdims=True) + EPSILON)
    normed = retained * inverse_rms
    normed_bf = normed.transpose(1, 0, 2).reshape(tokens, heads * value_width).astype(BF16)

    resid, normed_all = give_back(
        back_rows.reshape(n_sp, capacity, width), comb, og_q, normed_bf, n_tp
    )
    normed_grad = jnp.dot(resid, out_proj, preferred_element_type=F32)
    normed_grad = normed_grad.reshape(tokens, heads, value_width).transpose(1, 0, 2)
    grad = inverse_rms * (
        normed_grad - normed * jnp.mean(normed_grad * normed, axis=-1, keepdims=True)
    )
    grad_bf = grad.astype(BF16)
    inner_grad = ein("gwn,gwj->gnj", query_rot * decay, grad_bf).astype(BF16)
    resid_cols, grads_all = swap(resid, inner_grad, n_sp)
    future = weighted(grads_all, coming, ids > me).astype(BF16)
    score = fine("hiv,hjv->hij", grad, values) * mask
    query_portion = ein("hij,hjk->hik", score, key_bf) + decay * fine(
        "bpl,btl->bpt", grad, incoming
    )
    key_portion = ein("hij,hik->hjk", score, query_bf) + remaining * ein(
        "uxn,ubn->uxb", values, future
    )
    value_portion = ein("hij,hiv->hjv", weights, grad_bf) + remaining * ein(
        "bui,bim->bum", key_bf, future
    )
    query_grad = turn(query_portion, cosines, -sines, matrix).astype(BF16).transpose(1, 0, 2)
    key_grad = (
        (turn(key_portion, cosines, -sines, matrix) * scale).astype(BF16).transpose(1, 0, 2)
    )
    value_grad = value_portion.astype(BF16).transpose(1, 0, 2)
    proj_grad = mm(
        resid_cols.reshape(n_sp * tokens, -1), normed_all.reshape(n_sp * tokens, -1), 0, 0
    )
    return (
        gate_part[None],
        up_part[None],
        down_part[None],
        proj_grad,
        query_grad,
        key_grad,
        value_grad,
    )


def solution(mesh):
    in_specs = (
        P("sp", None),
        P("sp", None),
        P("sp", None),
        P("sp", None),
        P("sp", "tp", None),
        P("sp", "tp", None),
        P("sp", "tp", None),
        P("sp", "tp"),
        P(None, "tp"),
        P("sp", None, "tp"),
        P("sp", None, "tp"),
        P("sp", "tp", None),
    )
    out_specs = (
        P("sp", None, "tp"),
        P("sp", None, "tp"),
        P("sp", "tp", None),
        P("sp", "tp"),
        P("sp", "tp", None),
        P("sp", "tp", None),
        P("sp", "tp", None),
    )
    return jax.shard_map(
        per_device, mesh=mesh, in_specs=in_specs, out_specs=out_specs, check_vma=False
    )
```
